256 devices in a mesh: ep: 128 (over z, y, x), tp: 2 (over core).
Axes of the slice: x: 4, y: 4, z: 8, core: 2. Of those that a mesh axis runs over, the one named last changes fastest.
Arguments:
- tokens: bfloat16 [2048, 2048], P('ep', 'tp'), may hold values from -6 to 6
- mix_gain: float32 [2048], replicated, may hold values from 0.1 to 1.9
- input_weights: bfloat16 [2048, 1024], P(None, 'tp'), may hold values from -0.125 to 0.125
- decay_rates: float32 [64, 64], P('tp'), may hold values from 0.02 to 2
- frequencies: float32 [64, 64], P('tp'), may hold values from 0 to 200
- log_steps: float32 [64, 64], P('tp'), may hold values from -4.6 to -0.7
- input_real: float32 [64, 64, 16], P('tp'), may hold values from -1.5 to 1.5
- input_imaginary: float32 [64, 64, 16], P('tp'), may hold values from -1.5 to 1.5
- real_output_matrix: float32 [64, 16, 64], P('tp'), may hold values from -0.5 to 0.5
- imaginary_output_matrix: float32 [64, 16, 64], P('tp'), may hold values from -0.5 to 0.5
- skip_gain: float32 [1024], P('tp'), may hold values from -4 to 4
- real_state_part: float32 [2048, 64, 64], P('ep', 'tp'), may hold values from -6 to 6
- state_imaginary: float32 [2048, 64, 64], P('ep', 'tp'), may hold values from -6 to 6
- value_weights: bfloat16 [1024, 2048], P('tp'), may hold values from -0.1875 to 0.1875
- gate_weights: bfloat16 [1024, 2048], P('tp'), may hold values from -0.1875 to 0.1875
- expert_gain: float32 [2048], replicated, may hold values from 0.1 to 1.9
- routing: int32 [2048, 4], P('ep'), may hold values from 0 to 31, all different within a row; in each aligned block of 16 rows (0 to 15, 16 to 31, ...) at most 4 rows name the same one
- route_scores: float32 [2048, 4], P('ep'), may hold values from -2 to 2
- expert_gate: bfloat16 [128, 2048, 512], P('ep', None, 'tp'), may hold values from -0.375 to 0.375
- expert_up: bfloat16 [128, 2048, 512], P('ep', None, 'tp'), may hold values from -0.375 to 0.375
- expert_down: bfloat16 [128, 512, 2048], P('ep', 'tp'), may hold values from -0.03125 to 0.03125
Outputs:
- output: bfloat16 [2048, 2048], P('ep', 'tp')
- real_next: float32 [2048, 64, 64], P('ep', 'tp')
- imaginary_next: float32 [2048, 64, 64], P('ep', 'tp')
The draws below stay inside these ranges and needn't reach their ends.
Inputs may be any that keep to these rules, and one draw needn't show every extreme that they name: `routing`: each row names 4 different experts. In the rows of one index of ep, no expert is named by more than 4 rows, a bound that some block reaches.
All inputs are finite; a program needn't handle non-finite values.
Results may differ from the reference program's by a relative error of at most 0.014.
Values may be sent and summed in bfloat16 or wider, within the bound.
No kernel may reach another device: no remote copies, remote signals or barrier semaphores. Data moves between devices by JAX's collectives and lax.ppermute only.
A program may use at most 64 MiB of HBM per device.

```python
import math
import jax
import jax.numpy as jnp
import numpy as np
from jax import lax

D = 2048
FF = 2048
GROUP_CH = 16
STATE = 64
TOP_K = 4
SEQ_DEV = 16
S5W = 1024
GROUPS = 64
EXPERTS = 32
CAP = 4
SEQS = 2048
N_TP = 2


def steps_of(key, dims, pieces, low, high):
    def one(axis_at, parts):
        draws = jax.random.uniform(jax.random.fold_in(jax.random.fold_in(key, 6), axis_at), (parts,), jnp.float32, low / len(pieces), high / len(pieces))
        return jnp.repeat(jnp.exp(draws), dims[axis_at] // parts).reshape((-1,) + (1,) * (len(dims) - axis_at - 1))

    gain = one(*pieces[0])
    for cut in pieces[1:]:
        gain = gain * one(*cut)
    return gain


def assign_block(own_key, own, number, rows, number_of, top, bound, skew):
    ranking = jax.random.permutation(own_key, number_of)
    heavy_load, common = shares(number_of, rows * top, bound, skew, True), shares(number_of, rows * top, bound, skew, False)
    places = jnp.arange(number_of)

    def named(tallies, rotation):
        used = int((tallies > 0).sum())
        fixed = max(1, used // 4)
        shifted = fixed + (places - fixed + rotation * (used - fixed)) % max(1, number_of - fixed)
        return jnp.zeros((number_of,), jnp.int32).at[ranking[jnp.where(places < fixed, places, shifted)]].set(jnp.asarray(tallies, jnp.int32))

    tallies = jnp.where(number % 4 == 0, named(heavy_load, number // 4), named(common, number - number // 4 - 1))
    mixed = jax.random.permutation(jax.random.fold_in(own, 3), number_of)
    donor, sink = mixed[0:number_of // 2 * 2:2], mixed[1:number_of // 2 * 2:2]
    slack = jnp.minimum(tallies[donor] - 1, bound - tallies[sink]) // 2
    slack = jnp.where((donor == ranking[0]) | (sink == ranking[0]) | (tallies[sink] == 0), 0, jnp.maximum(slack, 0))
    shifted = jax.random.randint(jax.random.fold_in(own, 4), (number_of // 2,), 0, 1 << 20) % (slack + 1)
    tallies = tallies.at[donor].add(-shifted).at[sink].add(shifted)
    items = jnp.searchsorted(jnp.cumsum(tallies), jnp.arange(rows * top), side="right").astype(jnp.int32)
    listing = items.reshape(top, rows).T
    listing = listing[jax.random.permutation(jax.random.fold_in(own, 1), rows)]
    rotation = jax.random.randint(jax.random.fold_in(own, 2), (rows, 1), 0, top)
    return jnp.take_along_axis(listing, (jnp.arange(top)[None, :] + rotation) % top, axis=1)


def shares(number_of, total, bound, skew, full):
    weights = [(1 << 20) // math.isqrt(standing ** skew) + 1 for standing in range(1, number_of + 1)]
    largest = bound if full else min(bound, max(-(-total // number_of), total * weights[0] // sum(weights)))
    least = 1 if total - largest >= number_of - 1 else 0
    given, spare = [largest] + [least] * (number_of - 1), total - largest - least * (number_of - 1)
    while spare > 0:
        free = [i for i in range(1, number_of) if given[i] < largest] or [i for i in range(1, number_of) if given[i] < bound]
        whole, budget = sum([weights[i] for i in free]), spare
        for i in free:
            extra = min(bound - given[i], max(1, budget * weights[i] // whole), spare)
            given[i] = given[i] + extra
            spare = spare - extra
    return np.array(given)


def gaussian(key, shape, width, limit, split=(), kind=jnp.bfloat16):
    gain = steps_of(key, shape, split, -0.22, 0.18) if split else 1.0
    array = jax.random.normal(key, shape, jnp.float32) * width * gain
    return jnp.minimum(jnp.maximum(array, -limit), limit).astype(kind)


def setup_inputs(seed: int = 0) -> dict:
    keys = jax.random.split(jax.random.key(seed), 22)
    tokens = gaussian(keys[0], (SEQS, D), 1.0, 6.0, ((0, 128), (1, 2)))
    mix_gain = jnp.clip(1.0 + 0.18 * jax.random.normal(keys[1], (D,), jnp.float32), 0.1, 1.9)
    input_weights = gaussian(keys[2], (D, S5W), D ** -0.5, 0.125, ((1, 2),))
    decay_rates = jnp.clip(jnp.exp(math.log(2.0) - 4.6051702 * jax.random.uniform(keys[3], (GROUPS, STATE), jnp.float32) ** steps_of(keys[3], (GROUPS, STATE), ((0, 2),), -0.2, 0.2)), 0.02, 2.0)
    frequencies = jnp.clip(200.0 * jax.random.uniform(keys[4], (GROUPS, STATE), jnp.float32) ** steps_of(keys[4], (GROUPS, STATE), ((0, 2),), -0.2, 0.2), 0.0, 200.0)
    log_steps = jnp.clip(-4.6 + 3.8999999 * jax.random.uniform(keys[5], (GROUPS, STATE), jnp.float32) ** steps_of(keys[5], (GROUPS, STATE), ((0, 2),), -0.2, 0.2), -4.6, -0.7)
    input_real = gaussian(keys[6], (GROUPS, STATE, GROUP_CH), GROUP_CH ** -0.5, 1.5, ((0, 2),), jnp.float32)
    input_imaginary = gaussian(keys[7], (GROUPS, STATE, GROUP_CH), GROUP_CH ** -0.5, 1.5, ((0, 2),), jnp.float32)
    real_output_matrix = gaussian(keys[8], (GROUPS, GROUP_CH, STATE), (2 * STATE) ** -0.5, 0.5, ((0, 2),), jnp.float32)
    imaginary_output_matrix = gaussian(keys[9], (GROUPS, GROUP_CH, STATE), (2 * STATE) ** -0.5, 0.5, ((0, 2),), jnp.float32)
    skip_gain = gaussian(keys[10], (S5W,), 1.0, 4.0, ((0, 2),), jnp.float32)
    real_state_part = gaussian(keys[11], (SEQS, GROUPS, STATE), 1.0, 6.0, ((0, 128), (1, 2)), jnp.float32)
    state_imaginary = gaussian(keys[12], (SEQS, GROUPS, STATE), 1.0, 6.0, ((0, 128), (1, 2)), jnp.float32)
    value_weights = gaussian(keys[13], (S5W, D), S5W ** -0.5, 0.1875, ((0, 2),))
    gate_weights = gaussian(keys[14], (S5W, D), S5W ** -0.5, 0.1875, ((0, 2),))
    expert_gain = jnp.clip(1.0 + 0.18 * jax.random.normal(keys[15], (D,), jnp.float32), 0.1, 1.9)
    routing_keys = jax.random.split(jax.random.fold_in(keys[16], 1), SEQS // SEQ_DEV)
    routing_turns = jax.random.permutation(jax.random.fold_in(keys[16], 3), SEQS // SEQ_DEV)
    routing = jax.vmap(lambda own, number: assign_block(jax.random.fold_in(keys[16], 2), own, number, SEQ_DEV, EXPERTS, TOP_K, CAP, 2))(routing_keys, routing_turns).reshape((SEQS, TOP_K))
    route_scores = jnp.clip(jax.random.uniform(keys[17], (SEQS, TOP_K), jnp.float32, -2.0, 2.0) * steps_of(keys[17], (SEQS, TOP_K), ((0, 128),), -0.4, 0.0), -2.0, 2.0)
    expert_gate = gaussian(keys[18], (4 * EXPERTS, D, FF // 4), (D // 9) ** -0.5, 0.375, ((0, 128), (2, 2)))
    expert_up = gaussian(keys[19], (4 * EXPERTS, D, FF // 4), (D // 9) ** -0.5, 0.375, ((0, 128), (2, 2)))
    expert_down = gaussian(keys[20], (4 * EXPERTS, FF // 4, D), (16 * FF) ** -0.5, 0.03125, ((0, 128), (1, 2)))
    return dict(tokens=tokens, mix_gain=mix_gain, input_weights=input_weights, decay_rates=decay_rates, frequencies=frequencies, log_steps=log_steps, input_real=input_real, input_imaginary=input_imaginary, real_output_matrix=real_output_matrix, imaginary_output_matrix=imaginary_output_matrix, skip_gain=skip_gain, real_state_part=real_state_part, state_imaginary=state_imaginary, value_weights=value_weights, gate_weights=gate_weights, expert_gain=expert_gain, routing=routing, route_scores=route_scores, expert_gate=expert_gate, expert_up=expert_up, expert_down=expert_down)


epsilon = 1e-06
clamp_limit = 7.0
sigmoid_slope = 1.702
highest_precision = lax.Precision.HIGHEST

def rms_norm(values, gain_weights):
    energy = lax.optimization_barrier(jnp.mean(values * values, axis=-1, keepdims=True))
    return values * lax.rsqrt(energy + epsilon) * gain_weights

def state_update(inputs, decay_rates, frequencies, log_steps, input_real, input_imaginary, real_output_matrix, imaginary_output_matrix, skip_gain, real_state_part, state_imaginary):
    batch_rows = inputs.shape[0]
    groups, states, channel_list = input_real.shape
    grouped = inputs.reshape(batch_rows, groups, channel_list)
    step_sizes = jnp.exp(log_steps)
    magnitude = jnp.exp(-decay_rates * step_sizes)
    bar_real = magnitude * jnp.cos(frequencies * step_sizes)
    bar_imaginary = magnitude * jnp.sin(frequencies * step_sizes)
    minus_real = bar_real - 1.0
    modulus = decay_rates * decay_rates + frequencies * frequencies
    factor_real = (minus_real * -decay_rates + bar_imaginary * frequencies) / modulus
    factor_imaginary = (bar_imaginary * -decay_rates - minus_real * frequencies) / modulus
    drive_real = factor_real[..., None] * input_real - factor_imaginary[..., None] * input_imaginary
    drive_imaginary = factor_real[..., None] * input_imaginary + factor_imaginary[..., None] * input_real
    push_real = jnp.einsum('gpc,bgc->bgp', drive_real, grouped, precision=highest_precision)
    push_imaginary = jnp.einsum('gpc,bgc->bgp', drive_imaginary, grouped, precision=highest_precision)
    real_next = bar_real * real_state_part - bar_imaginary * state_imaginary + push_real
    imaginary_next = bar_real * state_imaginary + bar_imaginary * real_state_part + push_imaginary
    state_readout = jnp.einsum('ned,ond->one', real_output_matrix, real_next, precision=highest_precision) - jnp.einsum('ned,ond->one', imaginary_output_matrix, imaginary_next, precision=highest_precision)
    scanned = state_readout.reshape(batch_rows, groups * channel_list) + skip_gain * inputs
    return (scanned, real_next, imaginary_next)

def run_expert(operands):
    rows, gate_full, up_full, down_full = operands
    gate_pre = jnp.dot(rows, gate_full, preferred_element_type=jnp.float32)
    up_pre = jnp.dot(rows, up_full, preferred_element_type=jnp.float32)
    clipped_gate = jnp.minimum(gate_pre, clamp_limit)
    clipped_up = jnp.clip(up_pre, -clamp_limit, clamp_limit)
    hidden = (clipped_gate * jax.nn.sigmoid(sigmoid_slope * clipped_gate) * (clipped_up + 1.0)).astype(jnp.bfloat16)
    block_width = hidden.shape[1] // (4 * N_TP)
    summed = jnp.zeros((rows.shape[0], down_full.shape[1]), jnp.float32)
    for quarter in range(4):
        quarter_sum = jnp.zeros((rows.shape[0], down_full.shape[1]), jnp.float32)
        for half_id in range(N_TP):
            block_id = quarter * N_TP + half_id
            start = block_id * block_width
            partial_value = jnp.dot(hidden[:, start:start + block_width], down_full[start:start + block_width], preferred_element_type=jnp.float32).astype(jnp.bfloat16)
            partial_value = lax.optimization_barrier(partial_value)
            quarter_sum = quarter_sum + partial_value.astype(jnp.float32)
        rounded = lax.optimization_barrier(quarter_sum.astype(jnp.bfloat16))
        summed = summed + rounded.astype(jnp.float32)
    return summed

def reference(tokens, mix_gain, input_weights, decay_rates, frequencies, log_steps, input_real, input_imaginary, real_output_matrix, imaginary_output_matrix, skip_gain, real_state_part, state_imaginary, value_weights, gate_weights, expert_gain, routing, route_scores, expert_gate, expert_up, expert_down):
    stream = tokens.astype(jnp.float32)
    normed = rms_norm(stream, mix_gain).astype(jnp.bfloat16)
    inputs = jnp.dot(normed, input_weights, preferred_element_type=jnp.float32)
    scanned, real_next, imaginary_next = state_update(inputs, decay_rates, frequencies, log_steps, input_real, input_imaginary, real_output_matrix, imaginary_output_matrix, skip_gain, real_state_part, state_imaginary)
    activated = jax.nn.gelu(scanned, approximate=True).astype(jnp.bfloat16)
    share_width = activated.shape[1] // N_TP
    value_sum = jnp.zeros(stream.shape, jnp.float32)
    gate_sum = jnp.zeros(stream.shape, jnp.float32)
    for block_id in range(N_TP):
        start = block_id * share_width
        columns = activated[:, start:start + share_width]
        value_part = jnp.dot(columns, value_weights[start:start + share_width], preferred_element_type=jnp.float32).astype(jnp.bfloat16)
        gate_part = jnp.dot(columns, gate_weights[start:start + share_width], preferred_element_type=jnp.float32).astype(jnp.bfloat16)
        value_part, gate_part = lax.optimization_barrier((value_part, gate_part))
        value_sum = value_sum + value_part.astype(jnp.float32)
        gate_sum = gate_sum + gate_part.astype(jnp.float32)
    residual = stream + value_sum * jax.nn.sigmoid(gate_sum)
    expert_in = rms_norm(residual, expert_gain).astype(jnp.bfloat16)
    totals = jnp.exp(route_scores)
    route_weights = totals / lax.optimization_barrier(jnp.sum(totals, axis=1, keepdims=True))
    group_count = SEQS // SEQ_DEV
    per_group = routing.reshape(group_count, SEQ_DEV * TOP_K).astype(jnp.int32)
    member = (per_group[..., None] == jnp.arange(EXPERTS, dtype=jnp.int32)).astype(jnp.int32)
    earlier = jnp.cumsum(member, axis=1) - member
    slot_rank = lax.optimization_barrier(jnp.sum(earlier * member, axis=2))
    slot_index = (jnp.arange(group_count, dtype=jnp.int32)[:, None] * CAP + slot_rank).astype(jnp.int32)
    repeated = jnp.repeat(expert_in, TOP_K, axis=0).reshape(group_count, SEQ_DEV * TOP_K, D)
    buffers = jnp.zeros((EXPERTS, group_count * CAP, D), jnp.bfloat16).at[per_group, slot_index].set(repeated)
    gate_full = expert_gate.reshape(EXPERTS, 4, D, FF // 4).transpose(0, 2, 1, 3).reshape(EXPERTS, D, FF)
    up_full = expert_up.reshape(EXPERTS, 4, D, FF // 4).transpose(0, 2, 1, 3).reshape(EXPERTS, D, FF)
    down_full = expert_down.reshape(EXPERTS, FF, D)
    results = lax.map(run_expert, (buffers, gate_full, up_full, down_full))
    picked = results[per_group, slot_index].reshape(SEQS, TOP_K, D)
    mixture = lax.optimization_barrier(jnp.sum(route_weights[:, :, None] * picked, axis=1))
    output = (residual + mixture).astype(jnp.bfloat16)
    return (output, real_next, imaginary_next)
```

```python
import jax
import jax.numpy as jnp
from jax import lax
from jax.sharding import Mesh
from jax.sharding import PartitionSpec as P

epsilon = 1e-06
clamp_limit = 7.0
sigmoid_slope = 1.702
lanes = ("z", "y")


def shifted(array, axis, distance):
    size = lax.axis_size(axis)
    return lax.ppermute(array, axis, [(i, (i + distance) % size) for i in range(size)])


def in_order(own, peer, tp_index, dim):
    low = jnp.where(tp_index == 0, own, peer)
    high = jnp.where(tp_index == 0, peer, own)
    return jnp.concatenate([low, high], axis=dim)


def halves(array, tp_index):
    width = array.shape[1] // 2
    low, high = array[:, :width], array[:, width:]
    return jnp.where(tp_index == 0, low, high), jnp.where(tp_index == 0, high, low)


def rms_norm(values, gain_weights):
    energy = jnp.mean(values * values, axis=-1, keepdims=True)
    return values * lax.rsqrt(energy + epsilon) * gain_weights


def state_update(
    inputs,
    decay_rates,
    frequencies,
    log_steps,
    input_real,
    input_imaginary,
    real_output_matrix,
    imaginary_output_matrix,
    skip_gain,
    real_state_part,
    state_imaginary,
):
    batch_rows = inputs.shape[0]
    groups, states, channel_list = input_real.shape
    grouped = inputs.reshape(batch_rows, groups, channel_list)
    step_sizes = jnp.exp(log_steps)
    magnitude = jnp.exp(-decay_rates * step_sizes)
    bar_real = magnitude * jnp.cos(frequencies * step_sizes)
    bar_imaginary = magnitude * jnp.sin(frequencies * step_sizes)
    minus_real = bar_real - 1.0
    modulus = decay_rates * decay_rates + frequencies * frequencies
    factor_real = (minus_real * -decay_rates + bar_imaginary * frequencies) / modulus
    factor_imaginary = (bar_imaginary * -decay_rates - minus_real * frequencies) / modulus
    drive_real = factor_real[..., None] * input_real - factor_imaginary[..., None] * input_imaginary
    drive_imaginary = (
        factor_real[..., None] * input_imaginary + factor_imaginary[..., None] * input_real
    )
    push_real = jnp.einsum("gpc,bgc->bgp", drive_real, grouped)
    push_imaginary = jnp.einsum("gpc,bgc->bgp", drive_imaginary, grouped)
    real_next = bar_real * real_state_part - bar_imaginary * state_imaginary + push_real
    imaginary_next = bar_real * state_imaginary + bar_imaginary * real_state_part + push_imaginary
    state_readout = jnp.einsum("ned,ond->one", real_output_matrix, real_next) - jnp.einsum(
        "ned,ond->one", imaginary_output_matrix, imaginary_next
    )
    scanned = state_readout.reshape(batch_rows, groups * channel_list) + skip_gain * inputs
    return (scanned, real_next, imaginary_next)


def expert_quarter(rows, gate, up, down):
    gate_pre = jnp.dot(rows, gate, preferred_element_type=jnp.float32)
    up_pre = jnp.dot(rows, up, preferred_element_type=jnp.float32)
    clipped_gate = jnp.minimum(gate_pre, clamp_limit)
    clipped_up = jnp.clip(up_pre, -clamp_limit, clamp_limit)
    hidden = (
        clipped_gate * jax.nn.sigmoid(sigmoid_slope * clipped_gate) * (clipped_up + 1.0)
    ).astype(jnp.bfloat16)
    return jnp.dot(hidden, down, preferred_element_type=jnp.float32).astype(jnp.bfloat16)


def local(
    tokens,
    mix_gain,
    input_weights,
    decay_rates,
    frequencies,
    log_steps,
    input_real,
    input_imaginary,
    real_output_matrix,
    imaginary_output_matrix,
    skip_gain,
    real_state_part,
    state_imaginary,
    value_weights,
    gate_weights,
    expert_gain,
    routing,
    route_scores,
    expert_gate,
    expert_up,
    expert_down,
):
    tp_index = lax.axis_index("tp")
    stream = in_order(tokens, shifted(tokens, "tp", 1), tp_index, 1).astype(jnp.float32)
    normed = rms_norm(stream, mix_gain).astype(jnp.bfloat16)
    inputs = jnp.dot(normed, input_weights, preferred_element_type=jnp.float32)
    scanned, real_next, imaginary_next = state_update(
        inputs,
        decay_rates,
        frequencies,
        log_steps,
        input_real,
        input_imaginary,
        real_output_matrix,
        imaginary_output_matrix,
        skip_gain,
        real_state_part,
        state_imaginary,
    )
    activated = jax.nn.gelu(scanned, approximate=True).astype(jnp.bfloat16)
    value_part = jnp.dot(activated, value_weights, preferred_element_type=jnp.float32)
    gate_part = jnp.dot(activated, gate_weights, preferred_element_type=jnp.float32)
    parts = jnp.concatenate([value_part, gate_part], axis=0).astype(jnp.bfloat16)
    sums = parts.astype(jnp.float32) + shifted(parts, "tp", 1).astype(jnp.float32)
    row_count, top_count = routing.shape
    residual = stream + sums[:row_count] * jax.nn.sigmoid(sums[row_count:])
    expert_in = rms_norm(residual, expert_gain).astype(jnp.bfloat16)
    residual_own, _ = halves(residual, tp_index)
    expert_own, _ = halves(expert_in, tp_index)

    expert_count = lax.axis_size("z") * lax.axis_size("y")
    quarter_count = lax.axis_size("x")
    capacity = min(row_count, 2 * row_count * top_count // expert_count)
    route_list = routing.reshape(row_count * top_count)
    member = (route_list[:, None] == jnp.arange(expert_count, dtype=jnp.int32)[None, :]).astype(
        jnp.int32
    )
    earlier = jnp.cumsum(member, axis=0) - member
    slot_rank = jnp.sum(earlier * member, axis=1)
    slot_index = (route_list * capacity + slot_rank).reshape(row_count, top_count)
    slots = jnp.arange(expert_count * capacity, dtype=jnp.int32)
    chosen = slot_index[:, :, None] == slots[None, None, :]
    selector = jnp.any(chosen, axis=1).astype(jnp.bfloat16)
    totals = jnp.exp(route_scores)
    route_weights = totals / jnp.sum(totals, axis=1, keepdims=True)
    mixing = jnp.sum(jnp.where(chosen, route_weights[:, :, None], 0.0), axis=1)

    width = expert_own.shape[1]
    buffer = lax.dot_general(
        selector, expert_own, (((0,), (0,)), ((), ())), preferred_element_type=jnp.float32
    ).astype(jnp.bfloat16)
    arrived = lax.all_to_all(
        buffer.reshape(expert_count, capacity, width), lanes, split_axis=0, concat_axis=0, tiled=True
    ).reshape(expert_count * capacity, width)

    gate, up, down = expert_gate[0], expert_up[0], expert_down[0]
    total = None
    for distance in (0, 2, 1, 3):
        own = shifted(arrived, "x", distance) if distance else arrived
        rows = in_order(own, shifted(own, "tp", 1), tp_index, 1)
        partial = expert_quarter(rows, gate, up, down)
        kept, sent = halves(partial, tp_index)
        quarter = (kept.astype(jnp.float32) + shifted(sent, "tp", 1).astype(jnp.float32)).astype(
            jnp.bfloat16
        )
        back = shifted(quarter, "x", quarter_count - distance) if distance else quarter
        back = back.astype(jnp.float32)
        total = back if total is None else total + back
    returned = lax.all_to_all(
        total.astype(jnp.bfloat16).reshape(expert_count, capacity, width),
        lanes,
        split_axis=0,
        concat_axis=0,
        tiled=True,
    ).reshape(expert_count * capacity, width)
    mixture = jnp.dot(
        mixing,
        returned.astype(jnp.float32),
        precision=lax.Precision.HIGHEST,
        preferred_element_type=jnp.float32,
    )
    output = (residual_own + mixture).astype(jnp.bfloat16)
    return (output, real_next, imaginary_next)


def solution(mesh):
    torus = Mesh(mesh.devices.reshape(8, 4, 4, 2), ("z", "y", "x", "tp"))
    ep = ("z", "y", "x")
    in_specs = (
        P(ep, "tp"),
        P(),
        P(None, "tp"),
        P("tp", None),
        P("tp", None),
        P("tp", None),
        P("tp", None, None),
        P("tp", None, None),
        P("tp", None, None),
        P("tp", None, None),
        P("tp"),
        P(ep, "tp", None),
        P(ep, "tp", None),
        P("tp", None),
        P("tp", None),
        P(),
        P(ep, None),
        P(ep, None),
        P(ep, None, "tp"),
        P(ep, None, "tp"),
        P(ep, "tp", None),
    )
    out_specs = (P(ep, "tp"), P(ep, "tp", None), P(ep, "tp", None))
    return jax.shard_map(local, mesh=torus, in_specs=in_specs, out_specs=out_specs, check_vma=False)
```

```python
import jax
import jax.numpy as jnp
from jax import lax
from jax.experimental import pallas as pl
from jax.experimental.pallas import tpu as pltpu
from jax.sharding import Mesh
from jax.sharding import PartitionSpec as P

epsilon = 1e-06
clamp_limit = 7.0
sigmoid_slope = 1.702
capacity = 4
lanes = ("z", "y")


def shifted(array, axis, distance):
    size = lax.axis_size(axis)
    return lax.ppermute(array, axis, [(i, (i + distance) % size) for i in range(size)])


def transition(decay_rates, frequencies, log_steps):
    step_sizes = jnp.exp(log_steps)
    magnitude = jnp.exp(-decay_rates * step_sizes)
    bar_real = magnitude * jnp.cos(frequencies * step_sizes)
    bar_imaginary = magnitude * jnp.sin(frequencies * step_sizes)
    minus_real = bar_real - 1.0
    modulus = decay_rates * decay_rates + frequencies * frequencies
    factor_real = (minus_real * -decay_rates + bar_imaginary * frequencies) / modulus
    factor_imaginary = (bar_imaginary * -decay_rates - minus_real * frequencies) / modulus
    return bar_real, bar_imaginary, factor_real, factor_imaginary


def f32_dot(left, right):
    return jnp.dot(left, right, preferred_element_type=jnp.float32)


def dot_along_last(left, right):
    return lax.dot_general(
        left, right, (((1,), (1,)), ((), ())), preferred_element_type=jnp.float32
    )


def dot_along_first(left, right):
    return lax.dot_general(
        left, right, (((0,), (0,)), ((), ())), preferred_element_type=jnp.float32
    )


def both_halves(tp_ref, width):
    mine = pl.ds(pl.multiple_of(tp_ref[0] * width, width), width)
    theirs = pl.ds(pl.multiple_of((1 - tp_ref[0]) * width, width), width)
    return mine, theirs


def mixer_kernel(
    tp_ref,
    own_ref,
    peer_ref,
    gain_ref,
    input_weights_ref,
    bar_real_ref,
    bar_imaginary_ref,
    factor_real_ref,
    factor_imaginary_ref,
    input_real_ref,
    input_imaginary_ref,
    real_output_ref,
    imaginary_output_ref,
    skip_ref,
    real_ref,
    imaginary_ref,
    value_hbm,
    gate_hbm,
    expert_gate_hbm,
    expert_up_hbm,
    expert_down_hbm,
    parts_ref,
    real_next_ref,
    imaginary_next_ref,
    expert_gate_ref,
    expert_up_ref,
    expert_down_ref,
    value_ref,
    gate_ref,
    sems,
):
    copies = [
        pltpu.make_async_copy(source, target, sems.at[i])
        for i, (source, target) in enumerate(
            (
                (value_hbm, value_ref),
                (gate_hbm, gate_ref),
                (expert_gate_hbm, expert_gate_ref),
                (expert_up_hbm, expert_up_ref),
                (expert_down_hbm, expert_down_ref),
            )
        )
    ]
    for copy in copies:
        copy.start()
    rows, width = own_ref.shape
    mine, theirs = both_halves(tp_ref, width)
    own = own_ref[...].astype(jnp.float32)
    peer = peer_ref[...].astype(jnp.float32)
    energy = jnp.sum(own * own, axis=1, keepdims=True) + jnp.sum(peer * peer, axis=1, keepdims=True)
    scale = lax.rsqrt(energy / (2 * width) + epsilon)
    inputs = f32_dot(
        (own * scale * gain_ref[:, mine]).astype(jnp.bfloat16), input_weights_ref[mine, :]
    ) + f32_dot(
        (peer * scale * gain_ref[:, theirs]).astype(jnp.bfloat16), input_weights_ref[theirs, :]
    )
    groups, channels, states = input_real_ref.shape
    bundle = 128 // channels
    span = bundle * rows
    lane_group = lax.broadcasted_iota(jnp.int32, (span, 128), 1) // channels
    row_group = lax.broadcasted_iota(jnp.int32, (span, 128), 0) // rows
    same = lane_group == row_group
    scanned = []
    for j in range(groups // bundle):
        first = j * bundle
        block = inputs[:, j * 128 : (j + 1) * 128]
        spread = jnp.where(same, jnp.concatenate([block] * bundle, axis=0), 0.0).astype(jnp.bfloat16)
        members = pl.ds(first, bundle)
        flat = (bundle * channels, states)
        raw_real = f32_dot(spread, input_real_ref[members].reshape(flat).astype(jnp.bfloat16))
        raw_imaginary = f32_dot(
            spread, input_imaginary_ref[members].reshape(flat).astype(jnp.bfloat16)
        )
        real_rows, imaginary_rows = [], []
        for i in range(bundle):
            g = first + i
            line = slice(g, g + 1)
            push_a = raw_real[i * rows : (i + 1) * rows]
            push_b = raw_imaginary[i * rows : (i + 1) * rows]
            factor_real, factor_imaginary = factor_real_ref[line, :], factor_imaginary_ref[line, :]
            bar_real, bar_imaginary = bar_real_ref[line, :], bar_imaginary_ref[line, :]
            real, imaginary = real_ref[:, g, :], imaginary_ref[:, g, :]
            real_next = (
                bar_real * real
                - bar_imaginary * imaginary
                + (factor_real * push_a - factor_imaginary * push_b)
            )
            imaginary_next = (
                bar_real * imaginary
                + bar_imaginary * real
                + (factor_real * push_b + factor_imaginary * push_a)
            )
            real_next_ref[:, g, :] = real_next
            imaginary_next_ref[:, g, :] = imaginary_next
            real_rows.append(real_next)
            imaginary_rows.append(imaginary_next)
        flat = (bundle * channels, states)
        readout = dot_along_last(
            jnp.concatenate(real_rows, axis=0).astype(jnp.bfloat16),
            real_output_ref[members].reshape(flat).astype(jnp.bfloat16),
        ) - dot_along_last(
            jnp.concatenate(imaginary_rows, axis=0).astype(jnp.bfloat16),
            imaginary_output_ref[members].reshape(flat).astype(jnp.bfloat16),
        )
        readout = jnp.where(same, readout, 0.0).reshape(bundle, rows, 128)
        scanned.append(jnp.sum(readout, axis=0))
    scanned = jnp.concatenate(scanned, axis=1) + skip_ref[...] * inputs
    activated = jax.nn.gelu(scanned, approximate=True).astype(jnp.bfloat16)
    copies[0].wait()
    parts_ref[:rows, :] = f32_dot(activated, value_ref[...]).astype(jnp.bfloat16)
    copies[1].wait()
    parts_ref[rows:, :] = f32_dot(activated, gate_ref[...]).astype(jnp.bfloat16)
    for copy in copies[2:]:
        copy.wait()


def dispatch_kernel(
    tp_ref,
    own_ref,
    peer_ref,
    parts_ref,
    arrived_ref,
    gain_ref,
    routing_ref,
    scores_ref,
    residual_ref,
    buffer_ref,
    mixing_ref,
):
    rows, width = own_ref.shape
    mine, theirs = both_halves(tp_ref, width)

    def residual_of(stream_ref, columns):
        value = parts_ref[:rows, columns].astype(jnp.float32)
        value = value + arrived_ref[:rows, columns].astype(jnp.float32)
        gate = parts_ref[rows:, columns].astype(jnp.float32)
        gate = gate + arrived_ref[rows:, columns].astype(jnp.float32)
        return stream_ref[...].astype(jnp.float32) + value * jax.nn.sigmoid(gate)

    own = residual_of(own_ref, mine)
    peer = residual_of(peer_ref, theirs)
    residual_ref[...] = own
    energy = jnp.sum(own * own, axis=1, keepdims=True) + jnp.sum(peer * peer, axis=1, keepdims=True)
    scale = lax.rsqrt(energy / (2 * width) + epsilon)
    expert_own = (own * scale * gain_ref[:, mine]).astype(jnp.bfloat16)

    slots = buffer_ref.shape[0]
    choices = routing_ref.shape[0]
    slot = lax.broadcasted_iota(jnp.int32, (slots, rows), 0)
    scores = jnp.exp(scores_ref[...])
    weights = scores / jnp.sum(scores, axis=0, keepdims=True)
    member = jnp.zeros((slots, rows), jnp.float32)
    weight = jnp.zeros((slots, rows), jnp.float32)
    for k in range(choices):
        named = routing_ref[k : k + 1, :] == slot // capacity
        member = jnp.where(named, 1.0, member)
        weight = jnp.where(named, weights[k : k + 1, :], weight)
    earlier = lax.broadcasted_iota(jnp.int32, (rows, rows), 0) < lax.broadcasted_iota(
        jnp.int32, (rows, rows), 1
    )
    rank = f32_dot(
        member.astype(jnp.bfloat16), jnp.where(earlier, 1.0, 0.0).astype(jnp.bfloat16)
    )
    taken = rank == (slot % capacity).astype(jnp.float32)
    selector = jnp.where(taken, member, 0.0)
    mixing_ref[...] = jnp.where(taken, weight, 0.0)
    buffer_ref[...] = f32_dot(selector.astype(jnp.bfloat16), expert_own).astype(jnp.bfloat16)


def combine_kernel(residual_ref, mixing_ref, returned_ref, output_ref):
    mixing = mixing_ref[...]
    high = mixing.astype(jnp.bfloat16)
    low = (mixing - high.astype(jnp.float32)).astype(jnp.bfloat16)
    returned = returned_ref[...]
    mixture = dot_along_first(high, returned) + dot_along_first(low, returned)
    output_ref[...] = (residual_ref[...] + mixture).astype(output_ref.dtype)


def quarter_kernel(tp_ref, own_ref, peer_ref, gate_ref, up_ref, down_ref, kept_ref, sent_ref):
    mine, theirs = both_halves(tp_ref, own_ref.shape[1])

    def projected(weights_ref):
        return f32_dot(own_ref[...], weights_ref[0, mine, :]) + f32_dot(
            peer_ref[...], weights_ref[0, theirs, :]
        )

    clipped_gate = jnp.minimum(projected(gate_ref), clamp_limit)
    clipped_up = jnp.clip(projected(up_ref), -clamp_limit, clamp_limit)
    hidden = (
        clipped_gate * jax.nn.sigmoid(sigmoid_slope * clipped_gate) * (clipped_up + 1.0)
    ).astype(jnp.bfloat16)
    for out_ref, columns in ((sent_ref, theirs), (kept_ref, mine)):
        out_ref[...] = f32_dot(hidden, down_ref[0, :, columns]).astype(out_ref.dtype)


vmem = pl.BlockSpec(memory_space=pltpu.VMEM)
smem = pl.BlockSpec(memory_space=pltpu.SMEM)
hbm = pl.BlockSpec(memory_space=pl.ANY)


def local(
    tokens,
    mix_gain,
    input_weights,
    decay_rates,
    frequencies,
    log_steps,
    input_real,
    input_imaginary,
    real_output_matrix,
    imaginary_output_matrix,
    skip_gain,
    real_state_part,
    state_imaginary,
    value_weights,
    gate_weights,
    expert_gain,
    routing,
    route_scores,
    expert_gate,
    expert_up,
    expert_down,
):
    tp = lax.axis_index("tp").reshape(1)
    row_count, width = tokens.shape
    expert_count = lax.axis_size("z") * lax.axis_size("y")
    quarter_count = lax.axis_size("x")
    slots = expert_count * capacity

    def shape_of(array, dtype=None):
        return jax.ShapeDtypeStruct(array.shape, dtype or array.dtype)

    peer_tokens = shifted(tokens, "tp", 1)
    bars = transition(decay_rates, frequencies, log_steps)
    parts, real_next, imaginary_next, gate, up, down = pl.pallas_call(
        mixer_kernel,
        out_shape=(
            jax.ShapeDtypeStruct((2 * row_count, 2 * width), jnp.bfloat16),
            shape_of(real_state_part),
            shape_of(state_imaginary),
            pltpu.VMEM(expert_gate.shape, expert_gate.dtype),
            pltpu.VMEM(expert_up.shape, expert_up.dtype),
            pltpu.VMEM(expert_down.shape, expert_down.dtype),
        ),
        in_specs=[smem] + [vmem] * 15 + [hbm] * 5,
        out_specs=(vmem,) * 6,
        scratch_shapes=[
            pltpu.VMEM(value_weights.shape, value_weights.dtype),
            pltpu.VMEM(gate_weights.shape, gate_weights.dtype),
            pltpu.SemaphoreType.DMA((5,)),
        ],
        compiler_params=pltpu.CompilerParams(vmem_limit_bytes=24 << 20),
        name="mixer",
    )(
        tp,
        tokens,
        peer_tokens,
        mix_gain.reshape(1, -1),
        input_weights,
        *bars,
        jnp.swapaxes(input_real, 1, 2),
        jnp.swapaxes(input_imaginary, 1, 2),
        real_output_matrix,
        imaginary_output_matrix,
        skip_gain.reshape(1, -1),
        real_state_part,
        state_imaginary,
        value_weights,
        gate_weights,
        expert_gate,
        expert_up,
        expert_down,
    )
    residual_own, buffer, mixing = pl.pallas_call(
        dispatch_kernel,
        out_shape=(
            jax.ShapeDtypeStruct((row_count, width), jnp.float32),
            jax.ShapeDtypeStruct((slots, width), jnp.bfloat16),
            jax.ShapeDtypeStruct((slots, row_count), jnp.float32),
        ),
        in_specs=[smem] + [vmem] * 7,
        out_specs=(vmem,) * 3,
        compiler_params=pltpu.CompilerParams(vmem_limit_bytes=8 << 20),
        name="dispatch",
    )(
        tp,
        tokens,
        peer_tokens,
        parts,
        shifted(parts, "tp", 1),
        expert_gain.reshape(1, -1),
        routing.T,
        route_scores.T,
    )
    arrived = lax.all_to_all(
        buffer.reshape(expert_count, capacity, width), lanes, split_axis=0, concat_axis=0, tiled=True
    ).reshape(slots, width)

    total = None
    for distance in (0, 2, 1, 3):
        own = shifted(arrived, "x", distance) if distance else arrived
        peer = shifted(own, "tp", 1)
        kept, sent = pl.pallas_call(
            quarter_kernel,
            out_shape=(shape_of(own), shape_of(own)),
            in_specs=[smem] + [vmem] * 5,
            out_specs=(vmem, vmem),
            compiler_params=pltpu.CompilerParams(vmem_limit_bytes=8 << 20),
            name="quarter",
        )(tp, own, peer, gate, up, down)
        quarter = (kept.astype(jnp.float32) + shifted(sent, "tp", 1).astype(jnp.float32)).astype(
            jnp.bfloat16
        )
        back = shifted(quarter, "x", quarter_count - distance) if distance else quarter
        back = back.astype(jnp.float32)
        total = back if total is None else total + back
    returned = lax.all_to_all(
        total.astype(jnp.bfloat16).reshape(expert_count, capacity, width),
        lanes,
        split_axis=0,
        concat_axis=0,
        tiled=True,
    ).reshape(slots, width)
    output = pl.pallas_call(
        combine_kernel,
        out_shape=shape_of(tokens),
        in_specs=[vmem] * 3,
        out_specs=vmem,
        compiler_params=pltpu.CompilerParams(vmem_limit_bytes=4 << 20),
        name="combine",
    )(residual_own, mixing, returned)
    return (output, real_next, imaginary_next)


def solution(mesh):
    torus = Mesh(mesh.devices.reshape(8, 4, 4, 2), ("z", "y", "x", "tp"))
    ep = ("z", "y", "x")
    in_specs = (
        P(ep, "tp"),
        P(),
        P(None, "tp"),
        P("tp", None),
        P("tp", None),
        P("tp", None),
        P("tp", None, None),
        P("tp", None, None),
        P("tp", None, None),
        P("tp", None, None),
        P("tp"),
        P(ep, "tp", None),
        P(ep, "tp", None),
        P("tp", None),
        P("tp", None),
        P(),
        P(ep, None),
        P(ep, None),
        P(ep, None, "tp"),
        P(ep, None, "tp"),
        P(ep, "tp", None),
    )
    out_specs = (P(ep, "tp"), P(ep, "tp", None), P(ep, "tp", None))
    return jax.shard_map(local, mesh=torus, in_specs=in_specs, out_specs=out_specs, check_vma=False)
```

```python
import jax
import jax.numpy as jnp
from jax import lax
from jax.experimental import pallas as pl
from jax.experimental.pallas import tpu as pltpu
from jax.sharding import Mesh
from jax.sharding import PartitionSpec as P

epsilon = 1e-06
clamp_limit = 7.0
sigmoid_slope = 1.702
capacity = 4
held = 2
folds = 4
lanes = ("z", "y")


def shifted(array, axis, distance):
    size = lax.axis_size(axis)
    return lax.ppermute(array, axis, [(i, (i + distance) % size) for i in range(size)])


def f32_dot(left, right):
    return jnp.dot(left, right, preferred_element_type=jnp.float32)


def dot_along_last(left, right):
    return lax.dot_general(
        left, right, (((1,), (1,)), ((), ())), preferred_element_type=jnp.float32
    )


def dot_along_first(left, right):
    return lax.dot_general(
        left, right, (((0,), (0,)), ((), ())), preferred_element_type=jnp.float32
    )


def both_halves(tp_ref, width):
    mine = pl.ds(pl.multiple_of(tp_ref[0] * width, width), width)
    theirs = pl.ds(pl.multiple_of((1 - tp_ref[0]) * width, width), width)
    return mine, theirs


def loader_kernel(
    decay_hbm,
    frequencies_hbm,
    log_steps_hbm,
    weights_hbm,
    weights_ref,
    bar_real_ref,
    bar_imaginary_ref,
    factor_real_ref,
    factor_imaginary_ref,
    decay_ref,
    frequencies_ref,
    log_steps_ref,
    sems,
):
    small = [
        pltpu.make_async_copy(source, target, sems.at[i])
        for i, (source, target) in enumerate(
            (
                (decay_hbm, decay_ref),
                (frequencies_hbm, frequencies_ref),
                (log_steps_hbm, log_steps_ref),
            )
        )
    ]
    piece = weights_hbm.shape[0] // 4
    large = [
        pltpu.make_async_copy(
            weights_hbm.at[pl.ds(i * piece, piece)],
            weights_ref.at[pl.ds(i * piece, piece)],
            sems.at[3 + i],
        )
        for i in range(4)
    ]
    for copy in small + large:
        copy.start()
    for copy in small:
        copy.wait()
    decay_rates, frequencies = decay_ref[...], frequencies_ref[...]
    step_sizes = jnp.exp(log_steps_ref[...])
    magnitude = jnp.exp(-decay_rates * step_sizes)
    bar_real = magnitude * jnp.cos(frequencies * step_sizes)
    bar_imaginary = magnitude * jnp.sin(frequencies * step_sizes)
    minus_real = bar_real - 1.0
    modulus = decay_rates * decay_rates + frequencies * frequencies
    bar_real_ref[...] = bar_real
    bar_imaginary_ref[...] = bar_imaginary
    factor_real_ref[...] = (minus_real * -decay_rates + bar_imaginary * frequencies) / modulus
    factor_imaginary_ref[...] = (bar_imaginary * -decay_rates - minus_real * frequencies) / modulus
    for copy in large:
        copy.wait()


def mixer_kernel(
    tp_ref,
    own_ref,
    peer_ref,
    input_weights_ref,
    bar_real_ref,
    bar_imaginary_ref,
    factor_real_ref,
    factor_imaginary_ref,
    gain_hbm,
    input_real_hbm,
    input_imaginary_hbm,
    real_hbm,
    imaginary_hbm,
    real_output_hbm,
    imaginary_output_hbm,
    skip_hbm,
    value_hbm,
    gate_hbm,
    expert_gate_hbm,
    expert_up_hbm,
    expert_down_hbm,
    parts_ref,
    real_next_ref,
    imaginary_next_ref,
    expert_gate_ref,
    expert_up_ref,
    expert_down_ref,
    gain_ref,
    input_real_ref,
    input_imaginary_ref,
    real_ref,
    imaginary_ref,
    real_output_ref,
    imaginary_output_ref,
    skip_ref,
    value_ref,
    gate_ref,
    sems,
):
    sources = (
        gain_hbm,
        input_real_hbm,
        input_imaginary_hbm,
        real_hbm,
        imaginary_hbm,
        real_output_hbm,
        imaginary_output_hbm,
        skip_hbm,
        value_hbm,
        gate_hbm,
        expert_gate_hbm,
        expert_up_hbm,
        expert_down_hbm,
    )
    targets = (
        gain_ref,
        input_real_ref,
        input_imaginary_ref,
        real_ref,
        imaginary_ref,
        real_output_ref,
        imaginary_output_ref,
        skip_ref,
        value_ref,
        gate_ref,
        expert_gate_ref,
        expert_up_ref,
        expert_down_ref,
    )
    copies = [
        pltpu.make_async_copy(source, target, sems.at[i])
        for i, (source, target) in enumerate(zip(sources, targets))
    ]
    for copy in copies:
        copy.start()
    copies[0].wait()
    rows, width = own_ref.shape
    mine, theirs = both_halves(tp_ref, width)
    own = own_ref[...].astype(jnp.float32)
    peer = peer_ref[...].astype(jnp.float32)
    energy = jnp.sum(own * own, axis=1, keepdims=True) + jnp.sum(peer * peer, axis=1, keepdims=True)
    scale = lax.rsqrt(energy / (2 * width) + epsilon)
    inputs = f32_dot(
        (own * scale * gain_ref[:, mine]).astype(jnp.bfloat16), input_weights_ref[mine, :]
    ) + f32_dot(
        (peer * scale * gain_ref[:, theirs]).astype(jnp.bfloat16), input_weights_ref[theirs, :]
    )
    for copy in copies[1:8]:
        copy.wait()
    groups, channels, states = input_real_ref.shape
    bundle = 128 // channels
    span = bundle * rows
    lane_group = lax.broadcasted_iota(jnp.int32, (span, 128), 1) // channels
    row_group = lax.broadcasted_iota(jnp.int32, (span, 128), 0) // rows
    same = lane_group == row_group
    scanned = []
    for j in range(groups // bundle):
        first = j * bundle
        block = inputs[:, j * 128 : (j + 1) * 128]
        spread = jnp.where(same, jnp.concatenate([block] * bundle, axis=0), 0.0).astype(jnp.bfloat16)
        members = pl.ds(first, bundle)
        flat = (bundle * channels, states)
        raw_real = f32_dot(spread, input_real_ref[members].reshape(flat).astype(jnp.bfloat16))
        raw_imaginary = f32_dot(
            spread, input_imaginary_ref[members].reshape(flat).astype(jnp.bfloat16)
        )
        real_rows, imaginary_rows = [], []
        for i in range(bundle):
            g = first + i
            line = slice(g, g + 1)
            push_a = raw_real[i * rows : (i + 1) * rows]
            push_b = raw_imaginary[i * rows : (i + 1) * rows]
            factor_real, factor_imaginary = factor_real_ref[line, :], factor_imaginary_ref[line, :]
            bar_real, bar_imaginary = bar_real_ref[line, :], bar_imaginary_ref[line, :]
            real, imaginary = real_ref[:, g, :], imaginary_ref[:, g, :]
            real_next = (
                bar_real * real
                - bar_imaginary * imaginary
                + (factor_real * push_a - factor_imaginary * push_b)
            )
            imaginary_next = (
                bar_real * imaginary
                + bar_imaginary * real
                + (factor_real * push_b + factor_imaginary * push_a)
            )
            real_next_ref[:, g, :] = real_next
            imaginary_next_ref[:, g, :] = imaginary_next
            real_rows.append(real_next)
            imaginary_rows.append(imaginary_next)
        flat = (bundle * channels, states)
        readout = dot_along_last(
            jnp.concatenate(real_rows, axis=0).astype(jnp.bfloat16),
            real_output_ref[members].reshape(flat).astype(jnp.bfloat16),
        ) - dot_along_last(
            jnp.concatenate(imaginary_rows, axis=0).astype(jnp.bfloat16),
            imaginary_output_ref[members].reshape(flat).astype(jnp.bfloat16),
        )
        readout = jnp.where(same, readout, 0.0).reshape(bundle, rows, 128)
        scanned.append(jnp.sum(readout, axis=0))
    scanned = jnp.concatenate(scanned, axis=1) + skip_ref[...] * inputs
    activated = jax.nn.gelu(scanned, approximate=True).astype(jnp.bfloat16)
    copies[8].wait()
    parts_ref[:rows, :] = f32_dot(activated, value_ref[...]).astype(jnp.bfloat16)
    copies[9].wait()
    parts_ref[rows:, :] = f32_dot(activated, gate_ref[...]).astype(jnp.bfloat16)
    for copy in copies[10:]:
        copy.wait()


def dispatch_kernel(
    tp_ref,
    own_ref,
    peer_ref,
    parts_ref,
    arrived_ref,
    gain_ref,
    routing_ref,
    scores_ref,
    residual_ref,
    buffer_ref,
    mixing_ref,
):
    rows, width = own_ref.shape
    mine, theirs = both_halves(tp_ref, width)

    def residual_of(stream_ref, columns):
        value = parts_ref[:rows, columns].astype(jnp.float32)
        value = value + arrived_ref[:rows, columns].astype(jnp.float32)
        gate = parts_ref[rows:, columns].astype(jnp.float32)
        gate = gate + arrived_ref[rows:, columns].astype(jnp.float32)
        return stream_ref[...].astype(jnp.float32) + value * jax.nn.sigmoid(gate)

    own = residual_of(own_ref, mine)
    peer = residual_of(peer_ref, theirs)
    residual_ref[...] = own
    energy = jnp.sum(own * own, axis=1, keepdims=True) + jnp.sum(peer * peer, axis=1, keepdims=True)
    scale = lax.rsqrt(energy / (2 * width) + epsilon)

    lines, breadth = buffer_ref.shape
    choices = routing_ref.shape[0]
    line = lax.broadcasted_iota(jnp.int32, (lines, rows), 0)
    expert, place = line // (held * folds), tp_ref[0] * held + line // folds % held
    scores = jnp.exp(scores_ref[...])
    weights = scores / jnp.sum(scores, axis=0, keepdims=True)
    member = jnp.zeros((lines, rows), jnp.float32)
    weight = jnp.zeros((lines, rows), jnp.float32)
    for k in range(choices):
        named = routing_ref[k : k + 1, :] == expert
        member = jnp.where(named, 1.0, member)
        weight = jnp.where(named, weights[k : k + 1, :], weight)
    earlier = lax.broadcasted_iota(jnp.int32, (rows, rows), 0) < lax.broadcasted_iota(
        jnp.int32, (rows, rows), 1
    )
    rank = f32_dot(
        member.astype(jnp.bfloat16), jnp.where(earlier, 1.0, 0.0).astype(jnp.bfloat16)
    )
    taken = rank == place.astype(jnp.float32)
    mixing_ref[...] = jnp.where(taken, weight, 0.0)
    selector = jnp.where(taken, member, 0.0)
    per_half = width // breadth
    total = jnp.zeros((lines, breadth), jnp.float32)
    for half, columns, first in (
        (own, mine, tp_ref[0] * per_half),
        (peer, theirs, (1 - tp_ref[0]) * per_half),
    ):
        expert_in = (half * scale * gain_ref[:, columns]).astype(jnp.bfloat16)
        for i in range(per_half):
            chosen = jnp.where(line % folds == first + i, selector, 0.0).astype(jnp.bfloat16)
            total = total + f32_dot(chosen, expert_in[:, i * breadth : (i + 1) * breadth])
    buffer_ref[...] = total.astype(jnp.bfloat16)


def combine_kernel(tp_ref, residual_ref, mixing_ref, returned_ref, kept_ref, sent_ref):
    rows, width = residual_ref.shape
    lines, breadth = returned_ref.shape
    per_half = width // breadth
    line = lax.broadcasted_iota(jnp.int32, (lines, rows), 0)
    mixing = mixing_ref[...]
    returned = returned_ref[...]

    def mixture(fold):
        chosen = jnp.where(line % folds == fold, mixing, 0.0)
        high = chosen.astype(jnp.bfloat16)
        low = (chosen - high.astype(jnp.float32)).astype(jnp.bfloat16)
        return dot_along_first(high, returned) + dot_along_first(low, returned)

    for i in range(per_half):
        columns = slice(i * breadth, (i + 1) * breadth)
        sent = mixture((1 - tp_ref[0]) * per_half + i)
        sent_ref[:, columns] = sent.astype(sent_ref.dtype)
        kept_ref[:, columns] = residual_ref[:, columns] + mixture(tp_ref[0] * per_half + i)


def fold_selector(shape, line_dim, fold):
    line = lax.broadcasted_iota(jnp.int32, shape, line_dim)
    row = lax.broadcasted_iota(jnp.int32, shape, 1 - line_dim)
    return jnp.where(line == row * folds + fold, 1.0, 0.0).astype(jnp.bfloat16)


def quarter_kernel(*refs):
    gates, ups, downs = refs[:2], refs[2:4], refs[4:6]
    count = (len(refs) - 6) // 2
    row_refs, out_refs = refs[6 : 6 + count], refs[6 + count :]
    lines, breadth = row_refs[0].shape
    size = lines // folds
    unfolded = []
    for ref in row_refs:
        chunk = ref[...]
        pieces = [
            f32_dot(fold_selector((size, lines), 1, fold), chunk).astype(jnp.bfloat16)
            for fold in range(folds)
        ]
        unfolded.append(jnp.concatenate(pieces, axis=1))
    rows = jnp.concatenate(unfolded, axis=0)
    total = None
    for gate_ref, up_ref, down_ref in zip(gates, ups, downs):
        clipped_gate = jnp.minimum(f32_dot(rows, gate_ref[0]), clamp_limit)
        clipped_up = jnp.clip(f32_dot(rows, up_ref[0]), -clamp_limit, clamp_limit)
        hidden = (
            clipped_gate * jax.nn.sigmoid(sigmoid_slope * clipped_gate) * (clipped_up + 1.0)
        ).astype(jnp.bfloat16)
        partial = f32_dot(hidden, down_ref[0])
        total = partial if total is None else total + partial
    total = total.astype(jnp.bfloat16)
    for i, out_ref in enumerate(out_refs):
        part = total[i * size : (i + 1) * size]
        folded = jnp.zeros((lines, breadth), jnp.float32)
        for fold in range(folds):
            folded = folded + f32_dot(
                fold_selector((lines, size), 0, fold), part[:, fold * breadth : (fold + 1) * breadth]
            )
        out_ref[...] = folded.astype(out_ref.dtype)


vmem = pl.BlockSpec(memory_space=pltpu.VMEM)
smem = pl.BlockSpec(memory_space=pltpu.SMEM)
hbm = pl.BlockSpec(memory_space=pltpu.HBM)


def in_hbm(*arrays):
    return [pltpu.with_memory_space_constraint(array, pltpu.HBM) for array in arrays]


def local(
    tokens,
    mix_gain,
    input_weights,
    decay_rates,
    frequencies,
    log_steps,
    input_real,
    input_imaginary,
    real_output_matrix,
    imaginary_output_matrix,
    skip_gain,
    real_state_part,
    state_imaginary,
    value_weights,
    gate_weights,
    expert_gain,
    routing,
    route_scores,
    expert_gate,
    expert_up,
    expert_down,
):
    tp = lax.axis_index("tp").reshape(1)
    row_count, width = tokens.shape
    expert_count = lax.axis_size("z") * lax.axis_size("y")
    quarter_count = lax.axis_size("x")
    lines = expert_count * held * folds
    breadth = 2 * width // folds

    def shape_of(array, dtype=None):
        return jax.ShapeDtypeStruct(array.shape, dtype or array.dtype)

    def scratch_of(array):
        return pltpu.VMEM(array.shape, array.dtype)

    peer_tokens = shifted(tokens, "tp", 1)
    loaded = pl.pallas_call(
        loader_kernel,
        out_shape=(scratch_of(input_weights),) + (scratch_of(decay_rates),) * 4,
        in_specs=[hbm] * 4,
        out_specs=(vmem,) * 5,
        scratch_shapes=[scratch_of(decay_rates)] * 3 + [pltpu.SemaphoreType.DMA((7,))],
        compiler_params=pltpu.CompilerParams(vmem_limit_bytes=8 << 20),
        name="loader",
    )(*in_hbm(decay_rates, frequencies, log_steps, input_weights))
    stored = (
        mix_gain.reshape(1, -1),
        jnp.swapaxes(input_real, 1, 2),
        jnp.swapaxes(input_imaginary, 1, 2),
        real_state_part,
        state_imaginary,
        real_output_matrix,
        imaginary_output_matrix,
        skip_gain.reshape(1, -1),
        value_weights,
        gate_weights,
    )
    experts = (expert_gate, expert_up, expert_down)
    parts, real_next, imaginary_next, *own_experts = pl.pallas_call(
        mixer_kernel,
        out_shape=(
            jax.ShapeDtypeStruct((2 * row_count, 2 * width), jnp.bfloat16),
            shape_of(real_state_part),
            shape_of(state_imaginary),
        )
        + tuple(scratch_of(array) for array in experts),
        in_specs=[smem] + [vmem] * 7 + [hbm] * 13,
        out_specs=(vmem,) * 6,
        scratch_shapes=[scratch_of(array) for array in stored] + [pltpu.SemaphoreType.DMA((13,))],
        compiler_params=pltpu.CompilerParams(vmem_limit_bytes=24 << 20),
        name="mixer",
    )(tp, tokens, peer_tokens, *loaded, *in_hbm(*stored, *experts))
    residual_own, buffer, mixing = pl.pallas_call(
        dispatch_kernel,
        out_shape=(
            jax.ShapeDtypeStruct((row_count, width), jnp.float32),
            jax.ShapeDtypeStruct((lines, breadth), jnp.bfloat16),
            jax.ShapeDtypeStruct((lines, row_count), jnp.float32),
        ),
        in_specs=[smem] + [vmem] * 7,
        out_specs=(vmem,) * 3,
        compiler_params=pltpu.CompilerParams(vmem_limit_bytes=8 << 20),
        name="dispatch",
    )(
        tp,
        tokens,
        peer_tokens,
        parts,
        shifted(parts, "tp", 1),
        expert_gain.reshape(1, -1),
        routing.T,
        route_scores.T,
    )
    buffer, *own_experts = lax.optimization_barrier((buffer, *own_experts))
    weights = []
    for array in own_experts:
        weights += [array, shifted(array, "tp", 1)]

    def over_experts(array):
        return lax.all_to_all(array, lanes, split_axis=0, concat_axis=0, tiled=True)

    def quarters(chunks):
        return pl.pallas_call(
            quarter_kernel,
            out_shape=(shape_of(buffer),) * len(chunks),
            in_specs=[vmem] * (6 + len(chunks)),
            out_specs=(vmem,) * len(chunks),
            compiler_params=pltpu.CompilerParams(vmem_limit_bytes=16 << 20),
            name="quarter",
        )(*weights, *chunks)

    arrived = over_experts(buffer)
    distances = (2, 1, 3)
    chunks = [shifted(arrived, "x", distance) for distance in distances]
    (own_part,) = quarters([arrived])
    own_part, *chunks = lax.optimization_barrier((own_part, *chunks))
    total = own_part.astype(jnp.float32)
    for distance, part in zip(distances, quarters(chunks)):
        total = total + shifted(part, "x", quarter_count - distance).astype(jnp.float32)
    returned = over_experts(total.astype(jnp.bfloat16))
    kept, sent = pl.pallas_call(
        combine_kernel,
        out_shape=(shape_of(tokens, jnp.float32), shape_of(tokens)),
        in_specs=[smem] + [vmem] * 3,
        out_specs=(vmem,) * 2,
        compiler_params=pltpu.CompilerParams(vmem_limit_bytes=4 << 20),
        name="combine",
    )(tp, residual_own, mixing, returned)
    output = (kept + shifted(sent, "tp", 1).astype(jnp.float32)).astype(tokens.dtype)
    return (output, real_next, imaginary_next)


def solution(mesh):
    torus = Mesh(mesh.devices.reshape(8, 4, 4, 2), ("z", "y", "x", "tp"))
    ep = ("z", "y", "x")
    in_specs = (
        P(ep, "tp"),
        P(),
        P(None, "tp"),
        P("tp", None),
        P("tp", None),
        P("tp", None),
        P("tp", None, None),
        P("tp", None, None),
        P("tp", None, None),
        P("tp", None, None),
        P("tp"),
        P(ep, "tp", None),
        P(ep, "tp", None),
        P("tp", None),
        P("tp", None),
        P(),
        P(ep, None),
        P(ep, None),
        P(ep, None, "tp"),
        P(ep, None, "tp"),
        P(ep, "tp", None),
    )
    out_specs = (P(ep, "tp"), P(ep, "tp", None), P(ep, "tp", None))
    return jax.shard_map(local, mesh=torus, in_specs=in_specs, out_specs=out_specs, check_vma=False)
```

```python
import jax
import jax.numpy as jnp
from jax import lax
from jax.experimental import pallas as pl
from jax.experimental.pallas import tpu as pltpu
from jax.sharding import Mesh
from jax.sharding import PartitionSpec as P

epsilon = 1e-06
clamp_limit = 7.0
sigmoid_slope = 1.702
capacity = 4
held = 2
folds = 4
lanes = ("z", "y")


def shifted(array, axis, distance):
    size = lax.axis_size(axis)
    return lax.ppermute(array, axis, [(i, (i + distance) % size) for i in range(size)])


def f32_dot(left, right):
    return jnp.dot(left, right, preferred_element_type=jnp.float32)


def dot_along_last(left, right):
    return lax.dot_general(
        left, right, (((1,), (1,)), ((), ())), preferred_element_type=jnp.float32
    )


def dot_along_first(left, right):
    return lax.dot_general(
        left, right, (((0,), (0,)), ((), ())), preferred_element_type=jnp.float32
    )


def both_halves(tp_ref, width):
    mine = pl.ds(pl.multiple_of(tp_ref[0] * width, width), width)
    theirs = pl.ds(pl.multiple_of((1 - tp_ref[0]) * width, width), width)
    return mine, theirs


def loader_kernel(tp_ref, decay_hbm, frequencies_hbm, log_steps_hbm, weights_hbm, *refs):
    count = (len(refs) - 9) // 2
    stored_hbms, outs = refs[:count], refs[count : 2 * count + 5]
    decay_ref, frequencies_ref, log_steps_ref, sems = refs[2 * count + 5 :]
    weights_ref, bar_real_ref, bar_imaginary_ref, factor_real_ref, factor_imaginary_ref = outs[:5]
    width = weights_ref.shape[0]
    piece = width // 2
    pairs = [
        (decay_hbm, decay_ref),
        (frequencies_hbm, frequencies_ref),
        (log_steps_hbm, log_steps_ref),
    ]
    pairs += [
        (
            weights_hbm.at[pl.ds(pl.multiple_of(tp_ref[0] * width + i * piece, piece), piece)],
            weights_ref.at[pl.ds(i * piece, piece)],
        )
        for i in range(2)
    ]
    pairs += zip(stored_hbms, outs[5:])
    copies = [
        pltpu.make_async_copy(source, target, sems.at[i])
        for i, (source, target) in enumerate(pairs)
    ]
    for copy in copies:
        copy.start()
    for copy in copies[:3]:
        copy.wait()
    decay_rates, frequencies = decay_ref[...], frequencies_ref[...]
    step_sizes = jnp.exp(log_steps_ref[...])
    magnitude = jnp.exp(-decay_rates * step_sizes)
    bar_real = magnitude * jnp.cos(frequencies * step_sizes)
    bar_imaginary = magnitude * jnp.sin(frequencies * step_sizes)
    minus_real = bar_real - 1.0
    modulus = decay_rates * decay_rates + frequencies * frequencies
    bar_real_ref[...] = bar_real
    bar_imaginary_ref[...] = bar_imaginary
    factor_real_ref[...] = (minus_real * -decay_rates + bar_imaginary * frequencies) / modulus
    factor_imaginary_ref[...] = (bar_imaginary * -decay_rates - minus_real * frequencies) / modulus
    for copy in copies[3:]:
        copy.wait()


def experts_kernel(gate_hbm, up_hbm, down_hbm, inward_ref, down_ref, sems):
    pairs = []
    for i, source in enumerate((gate_hbm, up_hbm)):
        half = source.shape[1] // 2
        for j in range(2):
            span = pl.ds(j * half, half)
            pairs.append((source.at[0, span], inward_ref.at[i, span]))
    half = down_hbm.shape[1] // 2
    for j in range(2):
        span = pl.ds(j * half, half)
        pairs.append((down_hbm.at[0, span], down_ref.at[0, span]))
    copies = [
        pltpu.make_async_copy(source, target, sems.at[i])
        for i, (source, target) in enumerate(pairs)
    ]
    for copy in copies:
        copy.start()
    for copy in copies:
        copy.wait()


def mixer_kernel(
    tp_ref,
    own_ref,
    peer_ref,
    own_weights_ref,
    bar_real_ref,
    bar_imaginary_ref,
    factor_real_ref,
    factor_imaginary_ref,
    gain_ref,
    input_real_ref,
    input_imaginary_ref,
    real_ref,
    imaginary_ref,
    real_output_ref,
    imaginary_output_ref,
    skip_ref,
    peer_weights_hbm,
    value_hbm,
    gate_hbm,
    parts_ref,
    real_next_ref,
    imaginary_next_ref,
    peer_weights_ref,
    value_ref,
    gate_ref,
    sems,
):
    start = pl.multiple_of((1 - tp_ref[0]) * own_ref.shape[1], own_ref.shape[1])
    piece = own_ref.shape[1] // 2
    pairs = [
        (
            peer_weights_hbm.at[pl.ds(start + i * piece, piece)],
            peer_weights_ref.at[pl.ds(i * piece, piece)],
        )
        for i in range(2)
    ]
    pairs += [(value_hbm, value_ref), (gate_hbm, gate_ref)]
    copies = [
        pltpu.make_async_copy(source, target, sems.at[i])
        for i, (source, target) in enumerate(pairs)
    ]
    for copy in copies:
        copy.start()
    rows, width = own_ref.shape
    mine, theirs = both_halves(tp_ref, width)
    own = own_ref[...].astype(jnp.float32)
    peer = peer_ref[...].astype(jnp.float32)
    energy = jnp.sum(own * own, axis=1, keepdims=True) + jnp.sum(peer * peer, axis=1, keepdims=True)
    scale = lax.rsqrt(energy / (2 * width) + epsilon)
    inputs = f32_dot((own * scale * gain_ref[:, mine]).astype(jnp.bfloat16), own_weights_ref[...])
    copies[0].wait()
    copies[1].wait()
    inputs = inputs + f32_dot(
        (peer * scale * gain_ref[:, theirs]).astype(jnp.bfloat16), peer_weights_ref[...]
    )
    groups, channels, states = input_real_ref.shape
    bundle = 128 // channels
    span = bundle * rows
    lane_group = lax.broadcasted_iota(jnp.int32, (span, 128), 1) // channels
    row_group = lax.broadcasted_iota(jnp.int32, (span, 128), 0) // rows
    same = lane_group == row_group
    scanned = []
    for j in range(groups // bundle):
        first = j * bundle
        block = inputs[:, j * 128 : (j + 1) * 128]
        spread = jnp.where(same, jnp.concatenate([block] * bundle, axis=0), 0.0).astype(jnp.bfloat16)
        members = pl.ds(first, bundle)
        flat = (bundle * channels, states)
        raw_real = f32_dot(spread, input_real_ref[members].reshape(flat).astype(jnp.bfloat16))
        raw_imaginary = f32_dot(
            spread, input_imaginary_ref[members].reshape(flat).astype(jnp.bfloat16)
        )
        real_rows, imaginary_rows = [], []
        for i in range(bundle):
            g = first + i
            line = slice(g, g + 1)
            push_a = raw_real[i * rows : (i + 1) * rows]
            push_b = raw_imaginary[i * rows : (i + 1) * rows]
            factor_real, factor_imaginary = factor_real_ref[line, :], factor_imaginary_ref[line, :]
            bar_real, bar_imaginary = bar_real_ref[line, :], bar_imaginary_ref[line, :]
            real, imaginary = real_ref[:, g, :], imaginary_ref[:, g, :]
            real_next = (
                bar_real * real
                - bar_imaginary * imaginary
                + (factor_real * push_a - factor_imaginary * push_b)
            )
            imaginary_next = (
                bar_real * imaginary
                + bar_imaginary * real
                + (factor_real * push_b + factor_imaginary * push_a)
            )
            real_next_ref[:, g, :] = real_next
            imaginary_next_ref[:, g, :] = imaginary_next
            real_rows.append(real_next)
            imaginary_rows.append(imaginary_next)
        flat = (bundle * channels, states)
        readout = dot_along_last(
            jnp.concatenate(real_rows, axis=0).astype(jnp.bfloat16),
            real_output_ref[members].reshape(flat).astype(jnp.bfloat16),
        ) - dot_along_last(
            jnp.concatenate(imaginary_rows, axis=0).astype(jnp.bfloat16),
            imaginary_output_ref[members].reshape(flat).astype(jnp.bfloat16),
        )
        readout = jnp.where(same, readout, 0.0).reshape(bundle, rows, 128)
        scanned.append(jnp.sum(readout, axis=0))
    scanned = jnp.concatenate(scanned, axis=1) + skip_ref[...] * inputs
    activated = jax.nn.gelu(scanned, approximate=True).astype(jnp.bfloat16)
    copies[2].wait()
    parts_ref[:rows, :] = f32_dot(activated, value_ref[...]).astype(jnp.bfloat16)
    copies[3].wait()
    parts_ref[rows:, :] = f32_dot(activated, gate_ref[...]).astype(jnp.bfloat16)


def dispatch_kernel(
    tp_ref,
    own_ref,
    peer_ref,
    parts_ref,
    arrived_ref,
    gain_ref,
    routing_ref,
    scores_ref,
    residual_ref,
    buffer_ref,
    mixing_ref,
):
    rows, width = own_ref.shape
    mine, theirs = both_halves(tp_ref, width)

    def residual_of(stream_ref, columns):
        value = parts_ref[:rows, columns].astype(jnp.float32)
        value = value + arrived_ref[:rows, columns].astype(jnp.float32)
        gate = parts_ref[rows:, columns].astype(jnp.float32)
        gate = gate + arrived_ref[rows:, columns].astype(jnp.float32)
        return stream_ref[...].astype(jnp.float32) + value * jax.nn.sigmoid(gate)

    own = residual_of(own_ref, mine)
    peer = residual_of(peer_ref, theirs)
    residual_ref[...] = own
    energy = jnp.sum(own * own, axis=1, keepdims=True) + jnp.sum(peer * peer, axis=1, keepdims=True)
    scale = lax.rsqrt(energy / (2 * width) + epsilon)

    lines, breadth = buffer_ref.shape
    choices = routing_ref.shape[0]
    line = lax.broadcasted_iota(jnp.int32, (lines, rows), 0)
    expert, place = line // (held * folds), tp_ref[0] * held + line // folds % held
    scores = jnp.exp(scores_ref[...])
    weights = scores / jnp.sum(scores, axis=0, keepdims=True)
    member = jnp.zeros((lines, rows), jnp.float32)
    weight = jnp.zeros((lines, rows), jnp.float32)
    for k in range(choices):
        named = routing_ref[k : k + 1, :] == expert
        member = jnp.where(named, 1.0, member)
        weight = jnp.where(named, weights[k : k + 1, :], weight)
    earlier = lax.broadcasted_iota(jnp.int32, (rows, rows), 0) < lax.broadcasted_iota(
        jnp.int32, (rows, rows), 1
    )
    rank = f32_dot(
        member.astype(jnp.bfloat16), jnp.where(earlier, 1.0, 0.0).astype(jnp.bfloat16)
    )
    taken = rank == place.astype(jnp.float32)
    mixing_ref[...] = jnp.where(taken, weight, 0.0)
    selector = jnp.where(taken, member, 0.0)
    per_half = width // breadth
    total = jnp.zeros((lines, breadth), jnp.float32)
    for half, columns, first in (
        (own, mine, tp_ref[0] * per_half),
        (peer, theirs, (1 - tp_ref[0]) * per_half),
    ):
        expert_in = (half * scale * gain_ref[:, columns]).astype(jnp.bfloat16)
        for i in range(per_half):
            chosen = jnp.where(line % folds == first + i, selector, 0.0).astype(jnp.bfloat16)
            total = total + f32_dot(chosen, expert_in[:, i * breadth : (i + 1) * breadth])
    buffer_ref[...] = total.astype(jnp.bfloat16)


def combine_kernel(tp_ref, residual_ref, mixing_ref, returned_ref, kept_ref, sent_ref):
    rows, width = residual_ref.shape
    lines, breadth = returned_ref.shape
    per_half = width // breadth
    line = lax.broadcasted_iota(jnp.int32, (lines, rows), 0)
    mixing = mixing_ref[...]
    returned = returned_ref[...]

    def mixture(fold):
        chosen = jnp.where(line % folds == fold, mixing, 0.0)
        high = chosen.astype(jnp.bfloat16)
        low = (chosen - high.astype(jnp.float32)).astype(jnp.bfloat16)
        return dot_along_first(high, returned) + dot_along_first(low, returned)

    for i in range(per_half):
        columns = slice(i * breadth, (i + 1) * breadth)
        sent = mixture((1 - tp_ref[0]) * per_half + i)
        sent_ref[:, columns] = sent.astype(sent_ref.dtype)
        kept_ref[:, columns] = residual_ref[:, columns] + mixture(tp_ref[0] * per_half + i)


def fold_selector(lines):
    size = lines // folds
    spread = lax.broadcasted_iota(jnp.int32, (lines, lines), 0)
    line = lax.broadcasted_iota(jnp.int32, (lines, lines), 1)
    source = spread % size * folds + spread // size
    return jnp.where(line == source, 1.0, 0.0).astype(jnp.bfloat16)


def quarter_kernel(*refs):
    inwards, downs = refs[:2], refs[2:4]
    count = (len(refs) - 4) // 2
    row_refs, out_refs = refs[4 : 4 + count], refs[4 + count :]
    breadth = row_refs[0].shape[1]
    unfolded = []
    for ref in row_refs:
        size = ref.shape[0] // folds
        pieces = f32_dot(fold_selector(ref.shape[0]), ref[...]).astype(jnp.bfloat16)
        unfolded.append(
            jnp.concatenate([pieces[i * size : (i + 1) * size] for i in range(folds)], axis=1)
        )
    rows = jnp.concatenate(unfolded, axis=0)
    total = None
    for inward_ref, down_ref in zip(inwards, downs):
        clipped_gate = jnp.minimum(f32_dot(rows, inward_ref[0]), clamp_limit)
        clipped_up = jnp.clip(f32_dot(rows, inward_ref[1]), -clamp_limit, clamp_limit)
        hidden = (
            clipped_gate * jax.nn.sigmoid(sigmoid_slope * clipped_gate) * (clipped_up + 1.0)
        ).astype(jnp.bfloat16)
        partial = f32_dot(hidden, down_ref[0])
        total = partial if total is None else total + partial
    total = total.astype(jnp.bfloat16)
    first = 0
    for out_ref in out_refs:
        size = out_ref.shape[0] // folds
        part = total[first : first + size]
        first += size
        stacked = jnp.concatenate(
            [part[:, i * breadth : (i + 1) * breadth] for i in range(folds)], axis=0
        )
        out_ref[...] = dot_along_first(fold_selector(out_ref.shape[0]), stacked).astype(
            out_ref.dtype
        )


def split_kernel(whole_ref, low_ref, high_ref):
    half = low_ref.shape[0]
    low_ref[...] = whole_ref[:half, :]
    high_ref[...] = whole_ref[half:, :]


def sum_kernel(own_ref, right_ref, left_ref, low_ref, high_ref, total_ref):
    half = low_ref.shape[0]
    for i, ref in enumerate((low_ref, high_ref)):
        span = slice(i * half, (i + 1) * half)
        total = own_ref[span, :].astype(jnp.float32) + ref[...].astype(jnp.float32)
        total = total + right_ref[span, :].astype(jnp.float32)
        total = total + left_ref[span, :].astype(jnp.float32)
        total_ref[span, :] = total.astype(total_ref.dtype)


vmem = pl.BlockSpec(memory_space=pltpu.VMEM)
smem = pl.BlockSpec(memory_space=pltpu.SMEM)
hbm = pl.BlockSpec(memory_space=pltpu.HBM)


def in_hbm(*arrays):
    return [pltpu.with_memory_space_constraint(array, pltpu.HBM) for array in arrays]


def local(
    tokens,
    mix_gain,
    input_weights,
    decay_rates,
    frequencies,
    log_steps,
    input_real,
    input_imaginary,
    real_output_matrix,
    imaginary_output_matrix,
    skip_gain,
    real_state_part,
    state_imaginary,
    value_weights,
    gate_weights,
    expert_gain,
    routing,
    route_scores,
    expert_gate,
    expert_up,
    expert_down,
):
    tp = lax.axis_index("tp").reshape(1)
    row_count, width = tokens.shape
    expert_count = lax.axis_size("z") * lax.axis_size("y")
    quarter_count = lax.axis_size("x")
    lines = expert_count * held * folds
    breadth = 2 * width // folds

    def shape_of(array, dtype=None):
        return jax.ShapeDtypeStruct(array.shape, dtype or array.dtype)

    def scratch_of(array):
        return pltpu.VMEM(array.shape, array.dtype)

    peer_tokens = shifted(tokens, "tp", 1)
    stored = (
        mix_gain.reshape(1, -1),
        jnp.swapaxes(input_real, 1, 2),
        jnp.swapaxes(input_imaginary, 1, 2),
        real_state_part,
        state_imaginary,
        real_output_matrix,
        imaginary_output_matrix,
        skip_gain.reshape(1, -1),
    )
    half_weights = pltpu.VMEM((width, input_weights.shape[1]), input_weights.dtype)
    loaded = pl.pallas_call(
        loader_kernel,
        out_shape=(half_weights,)
        + (scratch_of(decay_rates),) * 4
        + tuple(scratch_of(array) for array in stored),
        in_specs=[smem] + [hbm] * (4 + len(stored)),
        out_specs=(vmem,) * (5 + len(stored)),
        scratch_shapes=[scratch_of(decay_rates)] * 3
        + [pltpu.SemaphoreType.DMA((5 + len(stored),))],
        compiler_params=pltpu.CompilerParams(vmem_limit_bytes=8 << 20),
        name="loader",
    )(tp, *in_hbm(decay_rates, frequencies, log_steps, input_weights, *stored))
    experts = (expert_gate, expert_up, expert_down)
    parts, real_next, imaginary_next = pl.pallas_call(
        mixer_kernel,
        out_shape=(
            jax.ShapeDtypeStruct((2 * row_count, 2 * width), jnp.bfloat16),
            shape_of(real_state_part),
            shape_of(state_imaginary),
        ),
        in_specs=[smem] + [vmem] * (7 + len(stored)) + [hbm] * 3,
        out_specs=(vmem,) * 3,
        scratch_shapes=[
            half_weights,
            scratch_of(value_weights),
            scratch_of(gate_weights),
            pltpu.SemaphoreType.DMA((4,)),
        ],
        compiler_params=pltpu.CompilerParams(vmem_limit_bytes=16 << 20),
        name="mixer",
    )(
        tp,
        tokens,
        peer_tokens,
        *loaded,
        *in_hbm(input_weights, value_weights, gate_weights),
    )
    arrived_parts = shifted(parts, "tp", 1)
    *experts, _ = lax.optimization_barrier((*experts, parts))
    own_experts = pl.pallas_call(
        experts_kernel,
        out_shape=(
            pltpu.VMEM((2, *expert_gate.shape[1:]), expert_gate.dtype),
            scratch_of(expert_down),
        ),
        in_specs=[hbm] * 3,
        out_specs=(vmem,) * 2,
        scratch_shapes=[pltpu.SemaphoreType.DMA((6,))],
        compiler_params=pltpu.CompilerParams(vmem_limit_bytes=4 << 20),
        name="experts",
    )(*in_hbm(*experts))
    tied, *own_experts = lax.optimization_barrier((tp, *own_experts))
    residual_own, buffer, mixing = pl.pallas_call(
        dispatch_kernel,
        out_shape=(
            jax.ShapeDtypeStruct((row_count, width), jnp.float32),
            jax.ShapeDtypeStruct((lines, breadth), jnp.bfloat16),
            jax.ShapeDtypeStruct((lines, row_count), jnp.float32),
        ),
        in_specs=[smem] + [vmem] * 7,
        out_specs=(vmem,) * 3,
        compiler_params=pltpu.CompilerParams(vmem_limit_bytes=8 << 20),
        name="dispatch",
    )(
        tied,
        tokens,
        peer_tokens,
        parts,
        arrived_parts,
        expert_gain.reshape(1, -1),
        routing.T,
        route_scores.T,
    )
    buffer, *own_experts = lax.optimization_barrier((buffer, *own_experts))
    weights = []
    for array in own_experts:
        weights += [array, shifted(array, "tp", 1)]

    def over_experts(array):
        return lax.all_to_all(array, lanes, split_axis=0, concat_axis=0, tiled=True)

    def quarters(chunks):
        return pl.pallas_call(
            quarter_kernel,
            out_shape=tuple(shape_of(chunk) for chunk in chunks),
            in_specs=[vmem] * (4 + len(chunks)),
            out_specs=(vmem,) * len(chunks),
            compiler_params=pltpu.CompilerParams(vmem_limit_bytes=16 << 20),
            name="quarter",
        )(*weights, *chunks)

    small = pltpu.CompilerParams(vmem_limit_bytes=4 << 20)
    arrived = over_experts(buffer)
    half = jax.ShapeDtypeStruct((lines // 2, breadth), jnp.bfloat16)
    low, high = pl.pallas_call(
        split_kernel,
        out_shape=(half, half),
        in_specs=[vmem],
        out_specs=(vmem, vmem),
        compiler_params=small,
        name="split",
    )(arrived)
    distances = (1, 3, 2, 2)
    chunks = [
        shifted(array, "x", distance)
        for array, distance in zip((arrived, arrived, low, high), distances)
    ]
    (own_part,) = quarters([arrived])
    own_part, *chunks = lax.optimization_barrier((own_part, *chunks))
    backs = [
        shifted(part, "x", quarter_count - distance)
        for distance, part in zip(distances, quarters(chunks))
    ]
    total = pl.pallas_call(
        sum_kernel,
        out_shape=shape_of(arrived),
        in_specs=[vmem] * 5,
        out_specs=vmem,
        compiler_params=small,
        name="sum",
    )(own_part, *backs)
    returned = over_experts(total)
    kept, sent = pl.pallas_call(
        combine_kernel,
        out_shape=(shape_of(tokens, jnp.float32), shape_of(tokens)),
        in_specs=[smem] + [vmem] * 3,
        out_specs=(vmem,) * 2,
        compiler_params=pltpu.CompilerParams(vmem_limit_bytes=4 << 20),
        name="combine",
    )(tp, residual_own, mixing, returned)
    output = (kept + shifted(sent, "tp", 1).astype(jnp.float32)).astype(tokens.dtype)
    return (output, real_next, imaginary_next)


def solution(mesh):
    torus = Mesh(mesh.devices.reshape(8, 4, 4, 2), ("z", "y", "x", "tp"))
    ep = ("z", "y", "x")
    in_specs = (
        P(ep, "tp"),
        P(),
        P(None, "tp"),
        P("tp", None),
        P("tp", None),
        P("tp", None),
        P("tp", None, None),
        P("tp", None, None),
        P("tp", None, None),
        P("tp", None, None),
        P("tp"),
        P(ep, "tp", None),
        P(ep, "tp", None),
        P("tp", None),
        P("tp", None),
        P(),
        P(ep, None),
        P(ep, None),
        P(ep, None, "tp"),
        P(ep, None, "tp"),
        P(ep, "tp", None),
    )
    out_specs = (P(ep, "tp"), P(ep, "tp", None), P(ep, "tp", None))
    return jax.shard_map(local, mesh=torus, in_specs=in_specs, out_specs=out_specs, check_vma=False)
```

```python
import jax
import jax.numpy as jnp
from jax import lax
from jax.experimental import pallas as pl
from jax.experimental.pallas import tpu as pltpu
from jax.sharding import Mesh
from jax.sharding import PartitionSpec as P

epsilon = 1e-06
clamp_limit = 7.0
sigmoid_slope = 1.702
capacity = 4
held = 2
folds = 4
lanes = ("z", "y")


def shifted(array, axis, distance):
    size = lax.axis_size(axis)
    return lax.ppermute(array, axis, [(i, (i + distance) % size) for i in range(size)])


def f32_dot(left, right):
    return jnp.dot(left, right, preferred_element_type=jnp.float32)


def dot_along_last(left, right):
    return lax.dot_general(
        left, right, (((1,), (1,)), ((), ())), preferred_element_type=jnp.float32
    )


def dot_along_first(left, right):
    return lax.dot_general(
        left, right, (((0,), (0,)), ((), ())), preferred_element_type=jnp.float32
    )


def both_halves(tp_ref, width):
    mine = pl.ds(pl.multiple_of(tp_ref[0] * width, width), width)
    theirs = pl.ds(pl.multiple_of((1 - tp_ref[0]) * width, width), width)
    return mine, theirs


def loader_kernel(tp_ref, decay_hbm, frequencies_hbm, log_steps_hbm, weights_hbm, *refs):
    count = (len(refs) - 9) // 2
    stored_hbms, outs = refs[:count], refs[count : 2 * count + 5]
    decay_ref, frequencies_ref, log_steps_ref, sems = refs[2 * count + 5 :]
    weights_ref, bar_real_ref, bar_imaginary_ref, factor_real_ref, factor_imaginary_ref = outs[:5]
    width = weights_ref.shape[0]
    piece = width // 2
    pairs = [
        (decay_hbm, decay_ref),
        (frequencies_hbm, frequencies_ref),
        (log_steps_hbm, log_steps_ref),
    ]
    pairs += [
        (
            weights_hbm.at[pl.ds(pl.multiple_of(tp_ref[0] * width + i * piece, piece), piece)],
            weights_ref.at[pl.ds(i * piece, piece)],
        )
        for i in range(2)
    ]
    pairs += zip(stored_hbms, outs[5:])
    copies = [
        pltpu.make_async_copy(source, target, sems.at[i])
        for i, (source, target) in enumerate(pairs)
    ]
    for copy in copies:
        copy.start()
    for copy in copies[:3]:
        copy.wait()
    decay_rates, frequencies = decay_ref[...], frequencies_ref[...]
    step_sizes = jnp.exp(log_steps_ref[...])
    magnitude = jnp.exp(-decay_rates * step_sizes)
    bar_real = magnitude * jnp.cos(frequencies * step_sizes)
    bar_imaginary = magnitude * jnp.sin(frequencies * step_sizes)
    minus_real = bar_real - 1.0
    modulus = decay_rates * decay_rates + frequencies * frequencies
    bar_real_ref[...] = bar_real
    bar_imaginary_ref[...] = bar_imaginary
    factor_real_ref[...] = (minus_real * -decay_rates + bar_imaginary * frequencies) / modulus
    factor_imaginary_ref[...] = (bar_imaginary * -decay_rates - minus_real * frequencies) / modulus
    for copy in copies[3:]:
        copy.wait()


def experts_kernel(gate_hbm, up_hbm, down_hbm, inward_ref, down_ref, sems):
    pairs = []
    for i, source in enumerate((gate_hbm, up_hbm)):
        half = source.shape[1] // 2
        for j in range(2):
            span = pl.ds(j * half, half)
            pairs.append((source.at[0, span], inward_ref.at[i, span]))
    half = down_hbm.shape[1] // 2
    for j in range(2):
        span = pl.ds(j * half, half)
        pairs.append((down_hbm.at[0, span], down_ref.at[0, span]))
    copies = [
        pltpu.make_async_copy(source, target, sems.at[i])
        for i, (source, target) in enumerate(pairs)
    ]
    for copy in copies:
        copy.start()
    for copy in copies:
        copy.wait()


def mixer_kernel(
    tp_ref,
    own_ref,
    peer_ref,
    own_weights_ref,
    bar_real_ref,
    bar_imaginary_ref,
    factor_real_ref,
    factor_imaginary_ref,
    gain_ref,
    input_real_ref,
    input_imaginary_ref,
    peer_weights_hbm,
    real_hbm,
    imaginary_hbm,
    real_output_hbm,
    imaginary_output_hbm,
    skip_hbm,
    value_hbm,
    gate_hbm,
    parts_ref,
    real_next_hbm,
    imaginary_next_hbm,
    real_next_ref,
    imaginary_next_ref,
    peer_weights_ref,
    real_ref,
    imaginary_ref,
    real_output_ref,
    imaginary_output_ref,
    skip_ref,
    value_ref,
    gate_ref,
    sems,
):
    start = pl.multiple_of((1 - tp_ref[0]) * own_ref.shape[1], own_ref.shape[1])
    piece = own_ref.shape[1] // 2
    pairs = [
        (
            peer_weights_hbm.at[pl.ds(start + i * piece, piece)],
            peer_weights_ref.at[pl.ds(i * piece, piece)],
        )
        for i in range(2)
    ]
    pairs += [
        (real_hbm, real_ref),
        (imaginary_hbm, imaginary_ref),
        (real_output_hbm, real_output_ref),
        (imaginary_output_hbm, imaginary_output_ref),
        (skip_hbm, skip_ref),
    ]
    part = value_hbm.shape[0] // 2
    for source, target in ((value_hbm, value_ref), (gate_hbm, gate_ref)):
        for i in range(2):
            span = pl.ds(i * part, part)
            pairs.append((source.at[span], target.at[span]))
    copies = [
        pltpu.make_async_copy(source, target, sems.at[i])
        for i, (source, target) in enumerate(pairs)
    ]
    for copy in copies:
        copy.start()
    rows, width = own_ref.shape
    mine, theirs = both_halves(tp_ref, width)
    own = own_ref[...].astype(jnp.float32)
    peer = peer_ref[...].astype(jnp.float32)
    energy = jnp.sum(own * own, axis=1, keepdims=True) + jnp.sum(peer * peer, axis=1, keepdims=True)
    scale = lax.rsqrt(energy / (2 * width) + epsilon)
    inputs = f32_dot((own * scale * gain_ref[:, mine]).astype(jnp.bfloat16), own_weights_ref[...])
    copies[0].wait()
    copies[1].wait()
    inputs = inputs + f32_dot(
        (peer * scale * gain_ref[:, theirs]).astype(jnp.bfloat16), peer_weights_ref[...]
    )
    groups, channels, states = input_real_ref.shape
    bundle = 128 // channels
    span = bundle * rows
    square = (span, 128)
    same = (
        lax.broadcasted_iota(jnp.int32, square, 1) // channels
        == lax.broadcasted_iota(jnp.int32, square, 0) % bundle
    )
    repeater = jnp.where(
        lax.broadcasted_iota(jnp.int32, (span, rows), 0) // bundle
        == lax.broadcasted_iota(jnp.int32, (span, rows), 1),
        1.0,
        0.0,
    ).astype(jnp.bfloat16)
    repeated = f32_dot(repeater, inputs.astype(jnp.bfloat16))
    for copy in copies[2:7]:
        copy.wait()
    flat, tile = (bundle * channels, states), (rows, bundle, states)
    scanned = []
    for j in range(groups // bundle):
        members = slice(j * bundle, (j + 1) * bundle)
        spread = jnp.where(same, repeated[:, j * 128 : (j + 1) * 128], 0.0).astype(jnp.bfloat16)
        push_a = f32_dot(spread, input_real_ref[members].reshape(flat).astype(jnp.bfloat16))
        push_b = f32_dot(spread, input_imaginary_ref[members].reshape(flat).astype(jnp.bfloat16))
        push_a, push_b = push_a.reshape(tile), push_b.reshape(tile)
        factor_real = factor_real_ref[members, :][None]
        factor_imaginary = factor_imaginary_ref[members, :][None]
        bar_real = bar_real_ref[members, :][None]
        bar_imaginary = bar_imaginary_ref[members, :][None]
        real, imaginary = real_ref[:, members, :], imaginary_ref[:, members, :]
        real_next = (
            bar_real * real
            - bar_imaginary * imaginary
            + (factor_real * push_a - factor_imaginary * push_b)
        )
        imaginary_next = (
            bar_real * imaginary
            + bar_imaginary * real
            + (factor_real * push_b + factor_imaginary * push_a)
        )
        real_next_ref[:, members, :] = real_next
        imaginary_next_ref[:, members, :] = imaginary_next
        readout = dot_along_last(
            real_next.reshape(span, states).astype(jnp.bfloat16),
            real_output_ref[members].reshape(flat).astype(jnp.bfloat16),
        ) - dot_along_last(
            imaginary_next.reshape(span, states).astype(jnp.bfloat16),
            imaginary_output_ref[members].reshape(flat).astype(jnp.bfloat16),
        )
        readout = jnp.where(same, readout, 0.0).reshape(rows, bundle, 128)
        scanned.append(jnp.sum(readout, axis=1))
    leaving = [
        pltpu.make_async_copy(source, target, sems.at[len(copies) + i])
        for i, (source, target) in enumerate(
            ((real_next_ref, real_next_hbm), (imaginary_next_ref, imaginary_next_hbm))
        )
    ]
    for copy in leaving:
        copy.start()
    scanned = jnp.concatenate(scanned, axis=1) + skip_ref[...] * inputs
    activated = jax.nn.gelu(scanned, approximate=True).astype(jnp.bfloat16)
    copies[7].wait()
    copies[8].wait()
    parts_ref[:rows, :] = f32_dot(activated, value_ref[...]).astype(jnp.bfloat16)
    copies[9].wait()
    copies[10].wait()
    parts_ref[rows:, :] = f32_dot(activated, gate_ref[...]).astype(jnp.bfloat16)
    for copy in leaving:
        copy.wait()


def dispatch_kernel(
    tp_ref,
    own_ref,
    peer_ref,
    parts_ref,
    arrived_ref,
    gain_ref,
    routing_ref,
    scores_ref,
    residual_ref,
    buffer_ref,
    mixing_ref,
):
    rows, width = own_ref.shape
    mine, theirs = both_halves(tp_ref, width)

    def residual_of(stream_ref, columns):
        value = parts_ref[:rows, columns].astype(jnp.float32)
        value = value + arrived_ref[:rows, columns].astype(jnp.float32)
        gate = parts_ref[rows:, columns].astype(jnp.float32)
        gate = gate + arrived_ref[rows:, columns].astype(jnp.float32)
        return stream_ref[...].astype(jnp.float32) + value * jax.nn.sigmoid(gate)

    own = residual_of(own_ref, mine)
    peer = residual_of(peer_ref, theirs)
    residual_ref[...] = own
    energy = jnp.sum(own * own, axis=1, keepdims=True) + jnp.sum(peer * peer, axis=1, keepdims=True)
    scale = lax.rsqrt(energy / (2 * width) + epsilon)

    lines, breadth = buffer_ref.shape
    choices = routing_ref.shape[0]
    line = lax.broadcasted_iota(jnp.int32, (lines, rows), 0)
    expert, place = line // (held * folds), tp_ref[0] * held + line // folds % held
    scores = jnp.exp(scores_ref[...])
    weights = scores / jnp.sum(scores, axis=0, keepdims=True)
    member = jnp.zeros((lines, rows), jnp.float32)
    weight = jnp.zeros((lines, rows), jnp.float32)
    for k in range(choices):
        named = routing_ref[k : k + 1, :] == expert
        member = jnp.where(named, 1.0, member)
        weight = jnp.where(named, weights[k : k + 1, :], weight)
    earlier = lax.broadcasted_iota(jnp.int32, (rows, rows), 0) < lax.broadcasted_iota(
        jnp.int32, (rows, rows), 1
    )
    rank = f32_dot(
        member.astype(jnp.bfloat16), jnp.where(earlier, 1.0, 0.0).astype(jnp.bfloat16)
    )
    taken = rank == place.astype(jnp.float32)
    mixing_ref[...] = jnp.where(taken, weight, 0.0)
    selector = jnp.where(taken, member, 0.0)
    per_half = width // breadth
    total = jnp.zeros((lines, breadth), jnp.float32)
    for half, columns, first in (
        (own, mine, tp_ref[0] * per_half),
        (peer, theirs, (1 - tp_ref[0]) * per_half),
    ):
        expert_in = (half * scale * gain_ref[:, columns]).astype(jnp.bfloat16)
        for i in range(per_half):
            chosen = jnp.where(line % folds == first + i, selector, 0.0).astype(jnp.bfloat16)
            total = total + f32_dot(chosen, expert_in[:, i * breadth : (i + 1) * breadth])
    buffer_ref[...] = total.astype(jnp.bfloat16)


def combine_kernel(tp_ref, residual_ref, mixing_ref, returned_ref, kept_ref, sent_ref):
    rows, width = residual_ref.shape
    lines, breadth = returned_ref.shape
    per_half = width // breadth
    line = lax.broadcasted_iota(jnp.int32, (lines, rows), 0)
    mixing = mixing_ref[...]
    returned = returned_ref[...]

    def mixture(fold):
        chosen = jnp.where(line % folds == fold, mixing, 0.0)
        high = chosen.astype(jnp.bfloat16)
        low = (chosen - high.astype(jnp.float32)).astype(jnp.bfloat16)
        return dot_along_first(high, returned) + dot_along_first(low, returned)

    for i in range(per_half):
        columns = slice(i * breadth, (i + 1) * breadth)
        sent = mixture((1 - tp_ref[0]) * per_half + i)
        sent_ref[:, columns] = sent.astype(sent_ref.dtype)
        kept_ref[:, columns] = residual_ref[:, columns] + mixture(tp_ref[0] * per_half + i)


def fold_selector(lines):
    size = lines // folds
    spread = lax.broadcasted_iota(jnp.int32, (lines, lines), 0)
    line = lax.broadcasted_iota(jnp.int32, (lines, lines), 1)
    source = spread % size * folds + spread // size
    return jnp.where(line == source, 1.0, 0.0).astype(jnp.bfloat16)


def quarter_kernel(*refs):
    inwards, downs = refs[:2], refs[2:4]
    count = (len(refs) - 4) // 2
    row_refs, out_refs = refs[4 : 4 + count], refs[4 + count :]
    breadth = row_refs[0].shape[1]
    unfolded = []
    for ref in row_refs:
        size = ref.shape[0] // folds
        pieces = f32_dot(fold_selector(ref.shape[0]), ref[...]).astype(jnp.bfloat16)
        unfolded.append(
            jnp.concatenate([pieces[i * size : (i + 1) * size] for i in range(folds)], axis=1)
        )
    rows = jnp.concatenate(unfolded, axis=0)
    total = None
    for inward_ref, down_ref in zip(inwards, downs):
        clipped_gate = jnp.minimum(f32_dot(rows, inward_ref[0]), clamp_limit)
        clipped_up = jnp.clip(f32_dot(rows, inward_ref[1]), -clamp_limit, clamp_limit)
        hidden = (
            clipped_gate * jax.nn.sigmoid(sigmoid_slope * clipped_gate) * (clipped_up + 1.0)
        ).astype(jnp.bfloat16)
        partial = f32_dot(hidden, down_ref[0])
        total = partial if total is None else total + partial
    total = total.astype(jnp.bfloat16)
    first = 0
    for out_ref in out_refs:
        size = out_ref.shape[0] // folds
        part = total[first : first + size]
        first += size
        stacked = jnp.concatenate(
            [part[:, i * breadth : (i + 1) * breadth] for i in range(folds)], axis=0
        )
        out_ref[...] = dot_along_first(fold_selector(out_ref.shape[0]), stacked).astype(
            out_ref.dtype
        )


def split_kernel(whole_ref, low_ref, high_ref):
    half = low_ref.shape[0]
    low_ref[...] = whole_ref[:half, :]
    high_ref[...] = whole_ref[half:, :]


def sum_kernel(own_ref, right_ref, left_ref, low_ref, high_ref, total_ref):
    half = low_ref.shape[0]
    for i, ref in enumerate((low_ref, high_ref)):
        span = slice(i * half, (i + 1) * half)
        total = own_ref[span, :].astype(jnp.float32) + ref[...].astype(jnp.float32)
        total = total + right_ref[span, :].astype(jnp.float32)
        total = total + left_ref[span, :].astype(jnp.float32)
        total_ref[span, :] = total.astype(total_ref.dtype)


vmem = pl.BlockSpec(memory_space=pltpu.VMEM)
smem = pl.BlockSpec(memory_space=pltpu.SMEM)
hbm = pl.BlockSpec(memory_space=pltpu.HBM)


def in_hbm(*arrays):
    return [pltpu.with_memory_space_constraint(array, pltpu.HBM) for array in arrays]


def local(
    tokens,
    mix_gain,
    input_weights,
    decay_rates,
    frequencies,
    log_steps,
    input_real,
    input_imaginary,
    real_output_matrix,
    imaginary_output_matrix,
    skip_gain,
    real_state_part,
    state_imaginary,
    value_weights,
    gate_weights,
    expert_gain,
    routing,
    route_scores,
    expert_gate,
    expert_up,
    expert_down,
):
    tp = lax.axis_index("tp").reshape(1)
    row_count, width = tokens.shape
    expert_count = lax.axis_size("z") * lax.axis_size("y")
    quarter_count = lax.axis_size("x")
    lines = expert_count * held * folds
    breadth = 2 * width // folds

    def shape_of(array, dtype=None):
        return jax.ShapeDtypeStruct(array.shape, dtype or array.dtype)

    def scratch_of(array):
        return pltpu.VMEM(array.shape, array.dtype)

    peer_tokens = shifted(tokens, "tp", 1)
    stored = (
        mix_gain.reshape(1, -1),
        jnp.swapaxes(input_real, 1, 2),
        jnp.swapaxes(input_imaginary, 1, 2),
    )
    streamed = (
        real_state_part,
        state_imaginary,
        real_output_matrix,
        imaginary_output_matrix,
        skip_gain.reshape(1, -1),
        value_weights,
        gate_weights,
    )
    half_weights = pltpu.VMEM((width, input_weights.shape[1]), input_weights.dtype)
    loaded = pl.pallas_call(
        loader_kernel,
        out_shape=(half_weights,)
        + (scratch_of(decay_rates),) * 4
        + tuple(scratch_of(array) for array in stored),
        in_specs=[smem] + [hbm] * (4 + len(stored)),
        out_specs=(vmem,) * (5 + len(stored)),
        scratch_shapes=[scratch_of(decay_rates)] * 3
        + [pltpu.SemaphoreType.DMA((5 + len(stored),))],
        compiler_params=pltpu.CompilerParams(vmem_limit_bytes=8 << 20),
        name="loader",
    )(tp, *in_hbm(decay_rates, frequencies, log_steps, input_weights, *stored))
    experts = (expert_gate, expert_up, expert_down)
    parts, real_next, imaginary_next = pl.pallas_call(
        mixer_kernel,
        out_shape=(
            jax.ShapeDtypeStruct((2 * row_count, 2 * width), jnp.bfloat16),
            shape_of(real_state_part),
            shape_of(state_imaginary),
        ),
        in_specs=[smem] + [vmem] * (7 + len(stored)) + [hbm] * 8,
        out_specs=(vmem, hbm, hbm),
        scratch_shapes=[scratch_of(real_state_part), scratch_of(state_imaginary), half_weights]
        + [scratch_of(array) for array in streamed]
        + [pltpu.SemaphoreType.DMA((13,))],
        compiler_params=pltpu.CompilerParams(vmem_limit_bytes=20 << 20),
        name="mixer",
    )(tp, tokens, peer_tokens, *loaded, *in_hbm(input_weights, *streamed))
    arrived_parts = shifted(parts, "tp", 1)
    *experts, _ = lax.optimization_barrier((*experts, parts))
    own_experts = pl.pallas_call(
        experts_kernel,
        out_shape=(
            pltpu.VMEM((2, *expert_gate.shape[1:]), expert_gate.dtype),
            scratch_of(expert_down),
        ),
        in_specs=[hbm] * 3,
        out_specs=(vmem,) * 2,
        scratch_shapes=[pltpu.SemaphoreType.DMA((6,))],
        compiler_params=pltpu.CompilerParams(vmem_limit_bytes=4 << 20),
        name="experts",
    )(*in_hbm(*experts))
    tied, *own_experts = lax.optimization_barrier((tp, *own_experts))
    residual_own, buffer, mixing = pl.pallas_call(
        dispatch_kernel,
        out_shape=(
            jax.ShapeDtypeStruct((row_count, width), jnp.float32),
            jax.ShapeDtypeStruct((lines, breadth), jnp.bfloat16),
            jax.ShapeDtypeStruct((lines, row_count), jnp.float32),
        ),
        in_specs=[smem] + [vmem] * 7,
        out_specs=(vmem,) * 3,
        compiler_params=pltpu.CompilerParams(vmem_limit_bytes=8 << 20),
        name="dispatch",
    )(
        tied,
        tokens,
        peer_tokens,
        parts,
        arrived_parts,
        expert_gain.reshape(1, -1),
        routing.T,
        route_scores.T,
    )
    buffer, *own_experts = lax.optimization_barrier((buffer, *own_experts))
    weights = []
    for array in own_experts:
        weights += [array, shifted(array, "tp", 1)]

    def over_experts(array):
        return lax.all_to_all(array, lanes, split_axis=0, concat_axis=0, tiled=True)

    def quarters(chunks):
        return pl.pallas_call(
            quarter_kernel,
            out_shape=tuple(shape_of(chunk) for chunk in chunks),
            in_specs=[vmem] * (4 + len(chunks)),
            out_specs=(vmem,) * len(chunks),
            compiler_params=pltpu.CompilerParams(vmem_limit_bytes=16 << 20),
            name="quarter",
        )(*weights, *chunks)

    small = pltpu.CompilerParams(vmem_limit_bytes=4 << 20)
    arrived = over_experts(buffer)
    half = jax.ShapeDtypeStruct((lines // 2, breadth), jnp.bfloat16)
    low, high = pl.pallas_call(
        split_kernel,
        out_shape=(half, half),
        in_specs=[vmem],
        out_specs=(vmem, vmem),
        compiler_params=small,
        name="split",
    )(arrived)
    distances = (1, 3, 2, 2)
    chunks = [
        shifted(array, "x", distance)
        for array, distance in zip((arrived, arrived, low, high), distances)
    ]
    (own_part,) = quarters([arrived])
    own_part, *chunks = lax.optimization_barrier((own_part, *chunks))
    backs = [
        shifted(part, "x", quarter_count - distance)
        for distance, part in zip(distances, quarters(chunks))
    ]
    total = pl.pallas_call(
        sum_kernel,
        out_shape=shape_of(arrived),
        in_specs=[vmem] * 5,
        out_specs=vmem,
        compiler_params=small,
        name="sum",
    )(own_part, *backs)
    returned = over_experts(total)
    kept, sent = pl.pallas_call(
        combine_kernel,
        out_shape=(shape_of(tokens, jnp.float32), shape_of(tokens)),
        in_specs=[smem] + [vmem] * 3,
        out_specs=(vmem,) * 2,
        compiler_params=pltpu.CompilerParams(vmem_limit_bytes=4 << 20),
        name="combine",
    )(tp, residual_own, mixing, returned)
    output = (kept + shifted(sent, "tp", 1).astype(jnp.float32)).astype(tokens.dtype)
    return (output, real_next, imaginary_next)


def solution(mesh):
    torus = Mesh(mesh.devices.reshape(8, 4, 4, 2), ("z", "y", "x", "tp"))
    ep = ("z", "y", "x")
    in_specs = (
        P(ep, "tp"),
        P(),
        P(None, "tp"),
        P("tp", None),
        P("tp", None),
        P("tp", None),
        P("tp", None, None),
        P("tp", None, None),
        P("tp", None, None),
        P("tp", None, None),
        P("tp"),
        P(ep, "tp", None),
        P(ep, "tp", None),
        P("tp", None),
        P("tp", None),
        P(),
        P(ep, None),
        P(ep, None),
        P(ep, None, "tp"),
        P(ep, None, "tp"),
        P(ep, "tp", None),
    )
    out_specs = (P(ep, "tp"), P(ep, "tp", None), P(ep, "tp", None))
    return jax.shard_map(local, mesh=torus, in_specs=in_specs, out_specs=out_specs, check_vma=False)
```

```python
import jax
import jax.numpy as jnp
from jax import lax
from jax.experimental import pallas as pl
from jax.experimental.pallas import tpu as pltpu
from jax.sharding import Mesh
from jax.sharding import PartitionSpec as P

epsilon = 1e-06
clamp_limit = 7.0
sigmoid_slope = 1.702
capacity = 4
held = 2
folds = 4
lanes = ("z", "y")


def shifted(array, axis, distance):
    size = lax.axis_size(axis)
    return lax.ppermute(array, axis, [(i, (i + distance) % size) for i in range(size)])


def f32_dot(left, right):
    return jnp.dot(left, right, preferred_element_type=jnp.float32)


def dot_along_last(left, right):
    return lax.dot_general(
        left, right, (((1,), (1,)), ((), ())), preferred_element_type=jnp.float32
    )


def dot_along_first(left, right):
    return lax.dot_general(
        left, right, (((0,), (0,)), ((), ())), preferred_element_type=jnp.float32
    )


def both_halves(tp_ref, width):
    mine = pl.ds(pl.multiple_of(tp_ref[0] * width, width), width)
    theirs = pl.ds(pl.multiple_of((1 - tp_ref[0]) * width, width), width)
    return mine, theirs


def loader_kernel(tp_ref, decay_hbm, frequencies_hbm, log_steps_hbm, weights_hbm, *refs):
    count = (len(refs) - 9) // 2
    stored_hbms, outs = refs[:count], refs[count : 2 * count + 5]
    decay_ref, frequencies_ref, log_steps_ref, sems = refs[2 * count + 5 :]
    weights_ref, bar_real_ref, bar_imaginary_ref, factor_real_ref, factor_imaginary_ref = outs[:5]
    width = weights_ref.shape[0]
    piece = width // 2
    pairs = [
        (decay_hbm, decay_ref),
        (frequencies_hbm, frequencies_ref),
        (log_steps_hbm, log_steps_ref),
    ]
    pairs += [
        (
            weights_hbm.at[pl.ds(pl.multiple_of(tp_ref[0] * width + i * piece, piece), piece)],
            weights_ref.at[pl.ds(i * piece, piece)],
        )
        for i in range(2)
    ]
    pairs += zip(stored_hbms, outs[5:])
    copies = [
        pltpu.make_async_copy(source, target, sems.at[i])
        for i, (source, target) in enumerate(pairs)
    ]
    for copy in copies:
        copy.start()
    for copy in copies[:3]:
        copy.wait()
    decay_rates, frequencies = decay_ref[...], frequencies_ref[...]
    step_sizes = jnp.exp(log_steps_ref[...])
    magnitude = jnp.exp(-decay_rates * step_sizes)
    bar_real = magnitude * jnp.cos(frequencies * step_sizes)
    bar_imaginary = magnitude * jnp.sin(frequencies * step_sizes)
    minus_real = bar_real - 1.0
    modulus = decay_rates * decay_rates + frequencies * frequencies
    bar_real_ref[...] = bar_real
    bar_imaginary_ref[...] = bar_imaginary
    factor_real_ref[...] = (minus_real * -decay_rates + bar_imaginary * frequencies) / modulus
    factor_imaginary_ref[...] = (bar_imaginary * -decay_rates - minus_real * frequencies) / modulus
    for copy in copies[3:]:
        copy.wait()


def experts_kernel(gate_hbm, up_hbm, down_hbm, inward_ref, down_ref, sems):
    pairs = []
    for i, source in enumerate((gate_hbm, up_hbm)):
        half = source.shape[1] // 2
        for j in range(2):
            span = pl.ds(j * half, half)
            pairs.append((source.at[0, span], inward_ref.at[i, span]))
    half = down_hbm.shape[1] // 2
    for j in range(2):
        span = pl.ds(j * half, half)
        pairs.append((down_hbm.at[0, span], down_ref.at[0, span]))
    copies = [
        pltpu.make_async_copy(source, target, sems.at[i])
        for i, (source, target) in enumerate(pairs)
    ]
    for copy in copies:
        copy.start()
    for copy in copies:
        copy.wait()


def mixer_kernel(
    tp_ref,
    own_ref,
    peer_ref,
    own_weights_ref,
    bar_real_ref,
    bar_imaginary_ref,
    factor_real_ref,
    factor_imaginary_ref,
    gain_ref,
    input_real_ref,
    input_imaginary_ref,
    peer_weights_hbm,
    real_hbm,
    imaginary_hbm,
    real_output_hbm,
    imaginary_output_hbm,
    skip_hbm,
    value_hbm,
    gate_hbm,
    parts_ref,
    real_next_hbm,
    imaginary_next_hbm,
    real_next_ref,
    imaginary_next_ref,
    peer_weights_ref,
    real_ref,
    imaginary_ref,
    real_output_ref,
    imaginary_output_ref,
    skip_ref,
    value_ref,
    gate_ref,
    sems,
):
    start = pl.multiple_of((1 - tp_ref[0]) * own_ref.shape[1], own_ref.shape[1])
    piece = own_ref.shape[1] // 2
    pairs = [
        (
            peer_weights_hbm.at[pl.ds(start + i * piece, piece)],
            peer_weights_ref.at[pl.ds(i * piece, piece)],
        )
        for i in range(2)
    ]
    pairs += [
        (real_hbm, real_ref),
        (imaginary_hbm, imaginary_ref),
        (real_output_hbm, real_output_ref),
        (imaginary_output_hbm, imaginary_output_ref),
        (skip_hbm, skip_ref),
    ]
    part = value_hbm.shape[0] // 2
    for source, target in ((value_hbm, value_ref), (gate_hbm, gate_ref)):
        for i in range(2):
            span = pl.ds(i * part, part)
            pairs.append((source.at[span], target.at[span]))
    copies = [
        pltpu.make_async_copy(source, target, sems.at[i])
        for i, (source, target) in enumerate(pairs)
    ]
    for copy in copies:
        copy.start()
    rows, width = own_ref.shape
    mine, theirs = both_halves(tp_ref, width)
    own = own_ref[...].astype(jnp.float32)
    peer = peer_ref[...].astype(jnp.float32)
    energy = jnp.sum(own * own, axis=1, keepdims=True) + jnp.sum(peer * peer, axis=1, keepdims=True)
    scale = lax.rsqrt(energy / (2 * width) + epsilon)
    inputs = f32_dot((own * scale * gain_ref[:, mine]).astype(jnp.bfloat16), own_weights_ref[...])
    copies[0].wait()
    copies[1].wait()
    inputs = inputs + f32_dot(
        (peer * scale * gain_ref[:, theirs]).astype(jnp.bfloat16), peer_weights_ref[...]
    )
    groups, channels, states = input_real_ref.shape
    bundle = 128 // channels
    span = bundle * rows
    square = (span, 128)
    same = (
        lax.broadcasted_iota(jnp.int32, square, 1) // channels
        == lax.broadcasted_iota(jnp.int32, square, 0) % bundle
    )
    repeater = jnp.where(
        lax.broadcasted_iota(jnp.int32, (span, rows), 0) // bundle
        == lax.broadcasted_iota(jnp.int32, (span, rows), 1),
        1.0,
        0.0,
    ).astype(jnp.bfloat16)
    repeated = f32_dot(repeater, inputs.astype(jnp.bfloat16))
    for copy in copies[2:7]:
        copy.wait()
    flat, tile = (bundle * channels, states), (rows, bundle, states)
    scanned = []
    for j in range(groups // bundle):
        members = slice(j * bundle, (j + 1) * bundle)
        spread = jnp.where(same, repeated[:, j * 128 : (j + 1) * 128], 0.0).astype(jnp.bfloat16)
        push_a = f32_dot(spread, input_real_ref[members].reshape(flat).astype(jnp.bfloat16))
        push_b = f32_dot(spread, input_imaginary_ref[members].reshape(flat).astype(jnp.bfloat16))
        push_a, push_b = push_a.reshape(tile), push_b.reshape(tile)
        factor_real = factor_real_ref[members, :][None]
        factor_imaginary = factor_imaginary_ref[members, :][None]
        bar_real = bar_real_ref[members, :][None]
        bar_imaginary = bar_imaginary_ref[members, :][None]
        real, imaginary = real_ref[:, members, :], imaginary_ref[:, members, :]
        real_next = (
            bar_real * real
            - bar_imaginary * imaginary
            + (factor_real * push_a - factor_imaginary * push_b)
        )
        imaginary_next = (
            bar_real * imaginary
            + bar_imaginary * real
            + (factor_real * push_b + factor_imaginary * push_a)
        )
        real_next_ref[:, members, :] = real_next
        imaginary_next_ref[:, members, :] = imaginary_next
        readout = dot_along_last(
            real_next.reshape(span, states).astype(jnp.bfloat16),
            real_output_ref[members].reshape(flat).astype(jnp.bfloat16),
        ) - dot_along_last(
            imaginary_next.reshape(span, states).astype(jnp.bfloat16),
            imaginary_output_ref[members].reshape(flat).astype(jnp.bfloat16),
        )
        readout = jnp.where(same, readout, 0.0).reshape(rows, bundle, 128)
        scanned.append(jnp.sum(readout, axis=1))
    leaving = [
        pltpu.make_async_copy(source, target, sems.at[len(copies) + i])
        for i, (source, target) in enumerate(
            ((real_next_ref, real_next_hbm), (imaginary_next_ref, imaginary_next_hbm))
        )
    ]
    for copy in leaving:
        copy.start()
    scanned = jnp.concatenate(scanned, axis=1) + skip_ref[...] * inputs
    activated = jax.nn.gelu(scanned, approximate=True).astype(jnp.bfloat16)
    copies[7].wait()
    copies[8].wait()
    parts_ref[:rows, :] = f32_dot(activated, value_ref[...]).astype(jnp.bfloat16)
    copies[9].wait()
    copies[10].wait()
    parts_ref[rows:, :] = f32_dot(activated, gate_ref[...]).astype(jnp.bfloat16)
    for copy in leaving:
        copy.wait()


def dispatch_kernel(
    tp_ref,
    own_ref,
    peer_ref,
    parts_ref,
    arrived_ref,
    gain_ref,
    routing_ref,
    scores_ref,
    residual_ref,
    buffer_ref,
    mixing_ref,
):
    rows, width = own_ref.shape
    mine, theirs = both_halves(tp_ref, width)

    def residual_of(stream_ref, columns):
        value = parts_ref[:rows, columns].astype(jnp.float32)
        value = value + arrived_ref[:rows, columns].astype(jnp.float32)
        gate = parts_ref[rows:, columns].astype(jnp.float32)
        gate = gate + arrived_ref[rows:, columns].astype(jnp.float32)
        return stream_ref[...].astype(jnp.float32) + value * jax.nn.sigmoid(gate)

    own = residual_of(own_ref, mine)
    peer = residual_of(peer_ref, theirs)
    residual_ref[...] = own
    energy = jnp.sum(own * own, axis=1, keepdims=True) + jnp.sum(peer * peer, axis=1, keepdims=True)
    scale = lax.rsqrt(energy / (2 * width) + epsilon)

    lines, breadth = buffer_ref.shape
    choices = routing_ref.shape[0]
    line = lax.broadcasted_iota(jnp.int32, (lines, rows), 0)
    expert, place = line // (held * folds), tp_ref[0] * held + line // folds % held
    scores = jnp.exp(scores_ref[...])
    weights = scores / jnp.sum(scores, axis=0, keepdims=True)
    member = jnp.zeros((lines, rows), jnp.float32)
    weight = jnp.zeros((lines, rows), jnp.float32)
    for k in range(choices):
        named = routing_ref[k : k + 1, :] == expert
        member = jnp.where(named, 1.0, member)
        weight = jnp.where(named, weights[k : k + 1, :], weight)
    earlier = lax.broadcasted_iota(jnp.int32, (rows, rows), 0) < lax.broadcasted_iota(
        jnp.int32, (rows, rows), 1
    )
    rank = f32_dot(
        member.astype(jnp.bfloat16), jnp.where(earlier, 1.0, 0.0).astype(jnp.bfloat16)
    )
    taken = rank == place.astype(jnp.float32)
    mixing_ref[...] = jnp.where(taken, weight, 0.0)
    selector = jnp.where(taken, member, 0.0)
    per_half = width // breadth
    total = jnp.zeros((lines, breadth), jnp.float32)
    for half, columns, first in (
        (own, mine, tp_ref[0] * per_half),
        (peer, theirs, (1 - tp_ref[0]) * per_half),
    ):
        expert_in = (half * scale * gain_ref[:, columns]).astype(jnp.bfloat16)
        for i in range(per_half):
            chosen = jnp.where(line % folds == first + i, selector, 0.0).astype(jnp.bfloat16)
            total = total + f32_dot(chosen, expert_in[:, i * breadth : (i + 1) * breadth])
    buffer_ref[...] = total.astype(jnp.bfloat16)


def combine_kernel(tp_ref, residual_ref, mixing_ref, returned_ref, kept_ref, sent_ref):
    rows, width = residual_ref.shape
    lines, breadth = returned_ref.shape
    per_half = width // breadth
    line = lax.broadcasted_iota(jnp.int32, (lines, rows), 0)
    mixing = mixing_ref[...]
    returned = returned_ref[...]

    def mixture(fold):
        chosen = jnp.where(line % folds == fold, mixing, 0.0)
        high = chosen.astype(jnp.bfloat16)
        low = (chosen - high.astype(jnp.float32)).astype(jnp.bfloat16)
        return dot_along_first(high, returned) + dot_along_first(low, returned)

    for i in range(per_half):
        columns = slice(i * breadth, (i + 1) * breadth)
        sent = mixture((1 - tp_ref[0]) * per_half + i)
        sent_ref[:, columns] = sent.astype(sent_ref.dtype)
        kept_ref[:, columns] = residual_ref[:, columns] + mixture(tp_ref[0] * per_half + i)


def fold_selector(lines):
    size = lines // folds
    spread = lax.broadcasted_iota(jnp.int32, (lines, lines), 0)
    line = lax.broadcasted_iota(jnp.int32, (lines, lines), 1)
    source = spread % size * folds + spread // size
    return jnp.where(line == source, 1.0, 0.0).astype(jnp.bfloat16)


def quarter_kernel(*refs):
    inwards, downs = refs[:2], refs[2:4]
    count = (len(refs) - 4) // 2
    row_refs, out_refs = refs[4 : 4 + count], refs[4 + count :]
    breadth = row_refs[0].shape[1]
    unfolded = []
    for ref in row_refs:
        size = ref.shape[0] // folds
        pieces = f32_dot(fold_selector(ref.shape[0]), ref[...]).astype(jnp.bfloat16)
        unfolded.append(
            jnp.concatenate([pieces[i * size : (i + 1) * size] for i in range(folds)], axis=1)
        )
    rows = jnp.concatenate(unfolded, axis=0)
    total = None
    for inward_ref, down_ref in zip(inwards, downs):
        clipped_gate = jnp.minimum(f32_dot(rows, inward_ref[0]), clamp_limit)
        clipped_up = jnp.clip(f32_dot(rows, inward_ref[1]), -clamp_limit, clamp_limit)
        hidden = (
            clipped_gate * jax.nn.sigmoid(sigmoid_slope * clipped_gate) * (clipped_up + 1.0)
        ).astype(jnp.bfloat16)
        partial = f32_dot(hidden, down_ref[0])
        total = partial if total is None else total + partial
    total = total.astype(jnp.bfloat16)
    first = 0
    for out_ref in out_refs:
        size = out_ref.shape[0] // folds
        part = total[first : first + size]
        first += size
        stacked = jnp.concatenate(
            [part[:, i * breadth : (i + 1) * breadth] for i in range(folds)], axis=0
        )
        out_ref[...] = dot_along_first(fold_selector(out_ref.shape[0]), stacked).astype(
            out_ref.dtype
        )


def sum_kernel(*refs):
    total = refs[0][...].astype(jnp.float32)
    for ref in refs[1:-1]:
        total = total + ref[...].astype(jnp.float32)
    refs[-1][...] = total.astype(refs[-1].dtype)


vmem = pl.BlockSpec(memory_space=pltpu.VMEM)
smem = pl.BlockSpec(memory_space=pltpu.SMEM)
hbm = pl.BlockSpec(memory_space=pltpu.HBM)


def in_hbm(*arrays):
    return [pltpu.with_memory_space_constraint(array, pltpu.HBM) for array in arrays]


def local(
    tokens,
    mix_gain,
    input_weights,
    decay_rates,
    frequencies,
    log_steps,
    input_real,
    input_imaginary,
    real_output_matrix,
    imaginary_output_matrix,
    skip_gain,
    real_state_part,
    state_imaginary,
    value_weights,
    gate_weights,
    expert_gain,
    routing,
    route_scores,
    expert_gate,
    expert_up,
    expert_down,
):
    tp = lax.axis_index("tp").reshape(1)
    row_count, width = tokens.shape
    expert_count = lax.axis_size("z") * lax.axis_size("y")
    quarter_count = lax.axis_size("x")
    lines = expert_count * held * folds
    breadth = 2 * width // folds

    def shape_of(array, dtype=None):
        return jax.ShapeDtypeStruct(array.shape, dtype or array.dtype)

    def scratch_of(array):
        return pltpu.VMEM(array.shape, array.dtype)

    peer_tokens = shifted(tokens, "tp", 1)
    stored = (
        mix_gain.reshape(1, -1),
        jnp.swapaxes(input_real, 1, 2),
        jnp.swapaxes(input_imaginary, 1, 2),
    )
    streamed = (
        real_state_part,
        state_imaginary,
        real_output_matrix,
        imaginary_output_matrix,
        skip_gain.reshape(1, -1),
        value_weights,
        gate_weights,
    )
    half_weights = pltpu.VMEM((width, input_weights.shape[1]), input_weights.dtype)
    loaded = pl.pallas_call(
        loader_kernel,
        out_shape=(half_weights,)
        + (scratch_of(decay_rates),) * 4
        + tuple(scratch_of(array) for array in stored),
        in_specs=[smem] + [hbm] * (4 + len(stored)),
        out_specs=(vmem,) * (5 + len(stored)),
        scratch_shapes=[scratch_of(decay_rates)] * 3
        + [pltpu.SemaphoreType.DMA((5 + len(stored),))],
        compiler_params=pltpu.CompilerParams(vmem_limit_bytes=8 << 20),
        name="loader",
    )(tp, *in_hbm(decay_rates, frequencies, log_steps, input_weights, *stored))
    experts = (expert_gate, expert_up, expert_down)
    parts, real_next, imaginary_next = pl.pallas_call(
        mixer_kernel,
        out_shape=(
            jax.ShapeDtypeStruct((2 * row_count, 2 * width), jnp.bfloat16),
            shape_of(real_state_part),
            shape_of(state_imaginary),
        ),
        in_specs=[smem] + [vmem] * (7 + len(stored)) + [hbm] * 8,
        out_specs=(vmem, hbm, hbm),
        scratch_shapes=[scratch_of(real_state_part), scratch_of(state_imaginary), half_weights]
        + [scratch_of(array) for array in streamed]
        + [pltpu.SemaphoreType.DMA((13,))],
        compiler_params=pltpu.CompilerParams(vmem_limit_bytes=20 << 20),
        name="mixer",
    )(tp, tokens, peer_tokens, *loaded, *in_hbm(input_weights, *streamed))
    arrived_parts = shifted(parts, "tp", 1)
    *experts, _ = lax.optimization_barrier((*experts, parts))
    own_experts = pl.pallas_call(
        experts_kernel,
        out_shape=(
            pltpu.VMEM((2, *expert_gate.shape[1:]), expert_gate.dtype),
            scratch_of(expert_down),
        ),
        in_specs=[hbm] * 3,
        out_specs=(vmem,) * 2,
        scratch_shapes=[pltpu.SemaphoreType.DMA((6,))],
        compiler_params=pltpu.CompilerParams(vmem_limit_bytes=4 << 20),
        name="experts",
    )(*in_hbm(*experts))
    tied, *own_experts = lax.optimization_barrier((tp, *own_experts))
    residual_own, buffer, mixing = pl.pallas_call(
        dispatch_kernel,
        out_shape=(
            jax.ShapeDtypeStruct((row_count, width), jnp.float32),
            jax.ShapeDtypeStruct((lines, breadth), jnp.bfloat16),
            jax.ShapeDtypeStruct((lines, row_count), jnp.float32),
        ),
        in_specs=[smem] + [vmem] * 7,
        out_specs=(vmem,) * 3,
        compiler_params=pltpu.CompilerParams(vmem_limit_bytes=8 << 20),
        name="dispatch",
    )(
        tied,
        tokens,
        peer_tokens,
        parts,
        arrived_parts,
        expert_gain.reshape(1, -1),
        routing.T,
        route_scores.T,
    )
    buffer, *own_experts = lax.optimization_barrier((buffer, *own_experts))
    weights = []
    for array in own_experts:
        weights += [array, shifted(array, "tp", 1)]

    def over_experts(array):
        return lax.all_to_all(array, lanes, split_axis=0, concat_axis=0, tiled=True)

    def quarters(chunks):
        return pl.pallas_call(
            quarter_kernel,
            out_shape=tuple(shape_of(chunk) for chunk in chunks),
            in_specs=[vmem] * (4 + len(chunks)),
            out_specs=(vmem,) * len(chunks),
            compiler_params=pltpu.CompilerParams(vmem_limit_bytes=16 << 20),
            name="quarter",
        )(*weights, *chunks)

    small = pltpu.CompilerParams(vmem_limit_bytes=4 << 20)
    arrived = over_experts(buffer)
    distances = (2, 1, 3)
    chunks = [shifted(arrived, "x", distance) for distance in distances]
    (own_part,) = quarters([arrived])
    *near, last = chunks
    own_part, last = lax.optimization_barrier((own_part, last))
    (last_part,) = quarters([last])
    last_back = shifted(last_part, "x", quarter_count - distances[-1])
    _, *near = lax.optimization_barrier((last_part, *near))
    backs = [
        shifted(part, "x", quarter_count - distance)
        for distance, part in zip(distances, quarters(near))
    ] + [last_back]
    total = pl.pallas_call(
        sum_kernel,
        out_shape=shape_of(arrived),
        in_specs=[vmem] * 4,
        out_specs=vmem,
        compiler_params=small,
        name="sum",
    )(own_part, *backs)
    returned = over_experts(total)
    kept, sent = pl.pallas_call(
        combine_kernel,
        out_shape=(shape_of(tokens, jnp.float32), shape_of(tokens)),
        in_specs=[smem] + [vmem] * 3,
        out_specs=(vmem,) * 2,
        compiler_params=pltpu.CompilerParams(vmem_limit_bytes=4 << 20),
        name="combine",
    )(tp, residual_own, mixing, returned)
    output = (kept + shifted(sent, "tp", 1).astype(jnp.float32)).astype(tokens.dtype)
    return (output, real_next, imaginary_next)


def solution(mesh):
    torus = Mesh(mesh.devices.reshape(8, 4, 4, 2), ("z", "y", "x", "tp"))
    ep = ("z", "y", "x")
    in_specs = (
        P(ep, "tp"),
        P(),
        P(None, "tp"),
        P("tp", None),
        P("tp", None),
        P("tp", None),
        P("tp", None, None),
        P("tp", None, None),
        P("tp", None, None),
        P("tp", None, None),
        P("tp"),
        P(ep, "tp", None),
        P(ep, "tp", None),
        P("tp", None),
        P("tp", None),
        P(),
        P(ep, None),
        P(ep, None),
        P(ep, None, "tp"),
        P(ep, None, "tp"),
        P(ep, "tp", None),
    )
    out_specs = (P(ep, "tp"), P(ep, "tp", None), P(ep, "tp", None))
    return jax.shard_map(local, mesh=torus, in_specs=in_specs, out_specs=out_specs, check_vma=False)
```
